512 devices in a mesh: sp: 64 (over z, y), tp: 8 (over x, core).
Axes of the slice: x: 4, y: 8, z: 8, core: 2. Of those that a mesh axis runs over, the one named last changes fastest.
Arguments:
- lookup_request_vectors: bfloat16 [16384, 1024], P('sp', 'tp'), may hold values from -6 to 6
- lookup_address_vectors: bfloat16 [16384, 1024], P('sp', 'tp'), may hold values from -6 to 6
- lookup_content_vectors: bfloat16 [16384, 1024], P('sp', 'tp'), may hold values from -6 to 6
- admission_preactivation: float32 [2, 16, 16384], P(None, 'tp', 'sp'), may hold values from -3 to 250
- retention_preactivation: float32 [2, 16, 16384], P(None, 'tp', 'sp'), may hold values from 0 to 20
- extra_decay_terms: float32 [2, 16, 16384], P(None, 'tp', 'sp'), may hold values from -0.6 to 0
- per_slot_rescale_factor: float32 [1024], P('tp'), may hold values from 0.1 to 1.9
- mixer_exit_matrix: bfloat16 [1024, 2048], P('tp'), may hold values from -0.1875 to 0.1875
- skip_path_activity: bfloat16 [16384, 2048], P(('sp', 'tp')), may hold values from -6 to 6
- mlp_rescale_factor: float32 [2048], replicated, may hold values from 0.1 to 1.9
- filter_widening_matrix: bfloat16 [2048, 5632], P('sp', 'tp'), may hold values from -0.125 to 0.125
- multiplier_widening_matrix: bfloat16 [2048, 5632], P('sp', 'tp'), may hold values from -0.125 to 0.125
- neighbour_filter_coefficients: float32 [3, 5632], P(None, 'tp'), may hold values from -3.5 to 3.5
- contracting_matrix: bfloat16 [5632, 2048], P('tp', 'sp'), may hold values from -0.078125 to 0.078125
Outputs:
- result: bfloat16 [16384, 2048], P(('sp', 'tp'))
The draws below stay inside these ranges and needn't reach their ends.
All inputs are finite; a program needn't handle non-finite values.
Results may differ from the reference program's by a relative error of at most 0.018.
Values may be sent and summed in bfloat16 or wider, within the bound.
No kernel may reach another device: no remote copies, remote signals or barrier semaphores. Data moves between devices by JAX's collectives and lax.ppermute only.
A program may use at most 64 MiB of HBM per device.

```python
import math
import jax
import jax.numpy as jnp
from jax import lax

D = 2048
HEADS = 16
HEAD_DIM = 64
FF = 5632
TOK_DEV = 256
BLOCK = 128
SEQ = 16384
ML_DIM = 1024
GROUP_FF = 704
N_TP = 8


def draw_admission_preactivation(key, part):
    key = jax.random.fold_in(key, 31)
    first = jax.random.fold_in(key, 0)
    shape = (2, HEADS, SEQ)
    return jnp.clip(jax.random.normal(first, shape, jnp.float32), -3.0, 3.0)


def draw_retention_preactivation(key, part):
    key = jax.random.fold_in(key, 47)
    first, second, third, fourth, fifth = jax.random.split(key, 5)
    slow_share = 0.5
    slow = jax.random.uniform(first, (2, HEADS, 1), jnp.float32) < slow_share
    fast_rate = jnp.exp(jax.random.uniform(second, (2, HEADS, 1), jnp.float32, math.log(1.0 / 50.0), math.log(1.0 / 30.0)))
    slow_rate = jnp.exp(jax.random.uniform(third, (2, HEADS, 1), jnp.float32, math.log(0.1), math.log(0.3))) / SEQ
    rate = jnp.where(slow, slow_rate, fast_rate)
    factor = jax.random.uniform(fourth, (2, 1, SEQ // TOK_DEV, 1), jnp.float32, math.log(0.5), math.log(2.0))
    factor = jnp.broadcast_to(factor, (2, 1, SEQ // TOK_DEV, TOK_DEV)).reshape(2, 1, SEQ)
    noise = jnp.clip(jax.random.normal(fifth, (2, HEADS, SEQ), jnp.float32) * 0.7, -1.75, 1.75)
    return -jnp.log(rate) - factor + noise


def draw_extra_decay_terms(key, part):
    key = jax.random.fold_in(key, 59)
    first, second = jax.random.split(key, 2)
    places = jax.random.randint(first, (2, 1, 3), 0, SEQ)
    depth = jax.random.uniform(second, (2, 1, 3), jnp.float32, math.log(0.6), math.log(0.8))
    positions = jnp.arange(SEQ)
    hits = positions[None, None, :, None] == places[:, :, None, :]
    added = jnp.sum(jnp.where(hits, depth[:, :, None, :], 0.0), axis=-1)
    return jnp.broadcast_to(added, (2, HEADS, SEQ)).astype(jnp.float32)


def block_levels(key, shape, cuts, smallest, largest):
    level = 1.0
    for dim, shards_of in cuts:
        draws = jax.random.uniform(jax.random.fold_in(jax.random.fold_in(key, 6), dim), (shards_of,), jnp.float32, smallest / len(cuts), largest / len(cuts))
        level = level * jnp.repeat(jnp.exp(draws), shape[dim] // shards_of).reshape((-1,) + (1,) * (len(shape) - 1 - dim))
    return level


def bell_draw(key, shape, scale, most, pieces=(), dtype=jnp.bfloat16):
    loudness = block_levels(key, shape, pieces, -0.22, 0.18) if pieces else 1.0
    entries = jax.random.normal(key, shape, jnp.float32) * scale * loudness
    return jnp.minimum(jnp.maximum(entries, -most), most).astype(dtype)


def setup_inputs(seed: int = 0) -> dict:
    splits = jax.random.split(jax.random.key(seed), 15)
    lookup_request_vectors = bell_draw(splits[0], (SEQ, ML_DIM), 1.0, 6.0, ((0, 64), (1, 8)))
    lookup_address_vectors = bell_draw(splits[1], (SEQ, ML_DIM), 1.0, 6.0, ((0, 64), (1, 8)))
    lookup_content_vectors = bell_draw(splits[2], (SEQ, ML_DIM), 1.0, 6.0, ((0, 64), (1, 8)))
    admission_preactivation = draw_admission_preactivation(jax.random.fold_in(splits[14], 71), 0)
    retention_preactivation = draw_retention_preactivation(jax.random.fold_in(splits[14], 71), 0)
    extra_decay_terms = draw_extra_decay_terms(jax.random.fold_in(splits[14], 71), 0)
    per_slot_rescale_factor = jnp.clip(1.0 + 0.18 * jax.random.normal(splits[6], (ML_DIM,), jnp.float32), 0.1, 1.9)
    mixer_exit_matrix = bell_draw(splits[7], (ML_DIM, D), ML_DIM ** -0.5, 0.1875, ((0, 8),))
    skip_path_activity = bell_draw(splits[8], (SEQ, D), 1.0, 6.0, ((0, 512),))
    mlp_rescale_factor = jnp.clip(1.0 + 0.18 * jax.random.normal(splits[9], (D,), jnp.float32), 0.1, 1.9)
    filter_widening_matrix = bell_draw(splits[10], (D, FF), D ** -0.5, 0.125, ((0, 64), (1, 8)))
    multiplier_widening_matrix = bell_draw(splits[11], (D, FF), D ** -0.5, 0.125, ((0, 64), (1, 8)))
    neighbour_filter_coefficients = bell_draw(splits[12], (3, FF), 3 ** -0.5, 3.5, ((1, 8),), jnp.float32)
    contracting_matrix = bell_draw(splits[13], (FF, D), FF ** -0.5, 0.078125, ((0, 8), (1, 64)))
    return dict(lookup_request_vectors=lookup_request_vectors, lookup_address_vectors=lookup_address_vectors, lookup_content_vectors=lookup_content_vectors, admission_preactivation=admission_preactivation, retention_preactivation=retention_preactivation, extra_decay_terms=extra_decay_terms, per_slot_rescale_factor=per_slot_rescale_factor, mixer_exit_matrix=mixer_exit_matrix, skip_path_activity=skip_path_activity, mlp_rescale_factor=mlp_rescale_factor, filter_widening_matrix=filter_widening_matrix, multiplier_widening_matrix=multiplier_widening_matrix, neighbour_filter_coefficients=neighbour_filter_coefficients, contracting_matrix=contracting_matrix)


precise_mode = lax.Precision.HIGHEST
epsilon = 1e-06

def block_step(state_in, block_in):
    memory, normal_sum, running_top = state_in
    query_blk, key_blk, value_blk, rate_blk, decay_blk = block_in
    length = decay_blk.shape[-1]
    cumul_decay = jnp.cumsum(decay_blk, axis=-1)
    block_total = cumul_decay[:, -1]
    lower = jnp.arange(length)[:, None] >= jnp.arange(length)[None, :]
    spread = cumul_decay[:, :, None] - cumul_decay[:, None, :] + rate_blk[:, None, :]
    spread = jnp.where(lower[None], spread, -jnp.inf)
    carried = cumul_decay + running_top[:, None]
    row_top = jnp.maximum(carried, lax.optimization_barrier(jnp.max(spread, axis=-1)))
    carry_weight = jnp.exp(carried - row_top)
    scores = jnp.einsum('hid,hjd->hij', query_blk, key_blk, precision=precise_mode) * jnp.exp(spread - row_top[:, :, None])
    numer = jnp.einsum('hij,hje->hie', scores, value_blk, precision=precise_mode)
    numer = numer + carry_weight[:, :, None] * jnp.einsum('hid,hde->hie', query_blk, memory, precision=precise_mode)
    denom = lax.optimization_barrier(jnp.sum(scores, axis=-1)) + carry_weight * jnp.einsum('hid,hd->hi', query_blk, normal_sum, precision=precise_mode)
    output = numer / jnp.maximum(jnp.abs(denom), jnp.exp(-row_top))[:, :, None]
    tail_weight = block_total[:, None] - cumul_decay + rate_blk
    new_top = jnp.maximum(block_total + running_top, lax.optimization_barrier(jnp.max(tail_weight, axis=-1)))
    fresh = jnp.exp(tail_weight - new_top[:, None])
    fade = jnp.exp(block_total + running_top - new_top)
    memory = fade[:, None, None] * memory + jnp.einsum('hjd,hje->hde', key_blk * fresh[:, :, None], value_blk, precision=precise_mode)
    normal_sum = fade[:, None] * normal_sum + jnp.einsum('hj,hjd->hd', fresh, key_blk, precision=precise_mode)
    return ((memory, normal_sum, new_top), output)

def run_blocks(query_heads, key_heads, value_heads, rate, decay, start_state):
    heads = query_heads.shape[0]
    length = query_heads.shape[1]
    count = length // BLOCK

    def to_blocks(array):
        return jnp.moveaxis(array.reshape((heads, count, BLOCK) + array.shape[2:]), 1, 0)
    inputs = tuple((to_blocks(array) for array in (query_heads, key_heads, value_heads, rate, decay)))
    _, outputs = lax.scan(block_step, start_state, inputs)
    return jnp.moveaxis(outputs, 0, 1).reshape(heads, length, -1)

def split_heads(array):
    return array.astype(jnp.float32).reshape(SEQ, HEADS, HEAD_DIM).transpose(1, 0, 2)

def reference(lookup_request_vectors, lookup_address_vectors, lookup_content_vectors, admission_preactivation, retention_preactivation, extra_decay_terms, per_slot_rescale_factor, mixer_exit_matrix, skip_path_activity, mlp_rescale_factor, filter_widening_matrix, multiplier_widening_matrix, neighbour_filter_coefficients, contracting_matrix):
    query_heads = split_heads(lookup_request_vectors)
    key_heads = split_heads(lookup_address_vectors) * HEAD_DIM ** (-0.5)
    value_heads = split_heads(lookup_content_vectors)
    retention_log_share = jax.nn.log_sigmoid(retention_preactivation) + extra_decay_terms
    start_state = (jnp.zeros((HEADS, HEAD_DIM, HEAD_DIM), jnp.float32), jnp.zeros((HEADS, HEAD_DIM), jnp.float32), jnp.zeros((HEADS,), jnp.float32))
    forward_out = run_blocks(query_heads, key_heads, value_heads, admission_preactivation[0], retention_log_share[0], start_state)
    backward_out = run_blocks(jnp.flip(query_heads, 1), jnp.flip(key_heads, 1), jnp.flip(value_heads, 1), jnp.flip(admission_preactivation[1], 1), jnp.flip(retention_log_share[1], 1), start_state)
    summed = forward_out + jnp.flip(backward_out, 1)
    scaled = summed * lax.rsqrt(lax.optimization_barrier(jnp.mean(summed * summed, axis=-1, keepdims=True)) + epsilon)
    scaled = scaled * per_slot_rescale_factor.reshape(HEADS, HEAD_DIM)[:, None, :]
    mixed = scaled.transpose(1, 0, 2).reshape(SEQ, ML_DIM).astype(jnp.bfloat16)
    projected = jnp.dot(mixed, mixer_exit_matrix, preferred_element_type=jnp.float32)
    middle = (skip_path_activity.astype(jnp.float32) + projected).astype(jnp.bfloat16)
    middle_wide = middle.astype(jnp.float32)
    normed = middle_wide * lax.rsqrt(lax.optimization_barrier(jnp.mean(middle_wide * middle_wide, axis=-1, keepdims=True)) + epsilon)
    normed = (normed * mlp_rescale_factor).astype(jnp.bfloat16)
    inner = jnp.dot(normed, filter_widening_matrix, preferred_element_type=jnp.float32).astype(jnp.bfloat16)
    gate = jnp.dot(normed, multiplier_widening_matrix, preferred_element_type=jnp.float32)
    padded = jnp.pad(inner.astype(jnp.float32), ((1, 1), (0, 0)))
    conv = neighbour_filter_coefficients[0] * padded[:-2] + neighbour_filter_coefficients[1] * padded[1:-1] + neighbour_filter_coefficients[2] * padded[2:]
    hidden = (jax.nn.gelu(conv) * gate).astype(jnp.bfloat16)
    total = jnp.zeros((SEQ, D), jnp.float32)
    for group in range(N_TP):
        first = group * GROUP_FF
        partial_value = jnp.dot(hidden[:, first:first + GROUP_FF], contracting_matrix[first:first + GROUP_FF], preferred_element_type=jnp.float32).astype(jnp.bfloat16)
        partial_value = lax.optimization_barrier(partial_value)
        total = total + partial_value.astype(jnp.float32)
    return (middle_wide + total).astype(jnp.bfloat16)
```

```python
import jax
import jax.numpy as jnp
from jax import lax
from jax.experimental import pallas as pl
from jax.experimental.pallas import tpu as pltpu
from jax.sharding import Mesh
from jax.sharding import PartitionSpec as P

HEAD_DIM = 64
SP = ("sp_0", "sp_1")
TP = ("x", "core")
SP_TP = SP + TP
EPS = 1e-06
FAR_BELOW = -1e30
STATE_ROWS = 136
HALF_ROWS = 72
LANES = 128
HIDDEN = 704
MAIN = 640
GATE_AT = MAIN + 128
DOWN_AT = GATE_AT + MAIN
PACKED = DOWN_AT + 768
FEED_STEPS = 4
ANY = pl.BlockSpec(memory_space=pl.ANY)
f32 = jnp.float32
bf16 = jnp.bfloat16
VMEM = pl.BlockSpec(memory_space=pltpu.VMEM)
SMEM = pl.BlockSpec(memory_space=pltpu.SMEM)


def three_parts(x):
    hi = x.astype(bf16)
    rest = x - hi.astype(f32)
    mid = rest.astype(bf16)
    low = (rest - mid.astype(f32)).astype(bf16)
    return hi, mid, low


def dot(a, b, dims=((1,), (0,))):
    return lax.dot_general(a, b, (dims, ((), ())), preferred_element_type=f32)


def dot_parts(parts, b, dims=((1,), (0,))):
    total = dot(parts[0], b, dims)
    for part in parts[1:]:
        total = total + dot(part, b, dims)
    return total


def iota(shape, dim):
    return lax.broadcasted_iota(jnp.int32, shape, dim)


def gate_rows(ref):
    place = iota((8, ref.shape[2]), 0)
    out = jnp.zeros((8, ref.shape[2]), f32)
    for d in range(2):
        for h in range(2):
            out = jnp.where(place == 2 * d + h, ref[d, h : h + 1, :], out)
    return out


def by_head(first, second, shape):
    return jnp.where(iota(shape, len(shape) - 1) < HEAD_DIM, first, second)


def packed_tail(rows):
    place = iota((8, LANES), 0)
    out = jnp.zeros((8, LANES), f32)
    for k, row in enumerate(rows):
        out = jnp.where(place == k, row, out)
    return out


def write_state(out_ref, memories, normals, totals, tops):
    tail = packed_tail([*normals, *totals, *tops])
    for copy in range(out_ref.shape[0]):
        for d in range(2):
            out_ref[copy, 64 * d : 64 * (d + 1), :] = memories[d]
        out_ref[copy, 128:, :] = tail


def write_halves(out_ref, here, memories, normals, totals, tops):
    tails = [packed_tail([normals[d], totals[d], tops[d]]) for d in range(2)]
    for copy in range(out_ref.shape[0]):
        later = copy > here
        out_ref[copy, :64, :] = jnp.where(later, memories[0], memories[1])
        out_ref[copy, 64:, :] = jnp.where(later, tails[0], tails[1])


def read_state(ref, j, d):
    if ref.shape[1] == HALF_ROWS:
        tail, at, step = ref[j, 64:, :], 0, 1
    else:
        tail, at, step = ref[j, 128:, :], d, 2
    return tuple(tail[at + k * step : at + k * step + 1] for k in range(3))


def summarize_kernel(key_ref, value_ref, rate_ref, decay_ref, out_ref):
    length = key_ref.shape[0]
    rate = gate_rows(rate_ref)
    decay = gate_rows(decay_ref)
    upper = (iota((length, length), 0) <= iota((length, length), 1)).astype(bf16)
    cumul = dot_parts(three_parts(decay), upper)
    total = cumul[:, length - 1 : length]
    is_forward = iota((8, length), 0) < 2
    weight = jnp.where(is_forward, total - cumul, cumul - decay) + rate
    top = jnp.max(weight, axis=1, keepdims=True)
    fresh = jnp.exp(weight - top)
    key_t = key_ref[...].astype(f32).T * HEAD_DIM ** (-0.5)
    value = value_ref[...]
    normal_all = dot_parts(three_parts(fresh), key_ref[...]) * HEAD_DIM ** (-0.5)
    memories, normals, totals, tops = [], [], [], []
    for d in range(2):
        a, b = 2 * d, 2 * d + 1
        spread = jnp.concatenate(
            [
                jnp.broadcast_to(fresh[a : a + 1], (HEAD_DIM, length)),
                jnp.broadcast_to(fresh[b : b + 1], (HEAD_DIM, length)),
            ],
            axis=0,
        )
        both = dot_parts(three_parts(key_t * spread), value)
        memories.append(by_head(both[:HEAD_DIM], both[HEAD_DIM:], (HEAD_DIM, LANES)))
        row = (1, LANES)
        normals.append(by_head(normal_all[a : a + 1], normal_all[b : b + 1], row))
        totals.append(by_head(total[a : a + 1], total[b : b + 1], row))
        tops.append(by_head(top[a : a + 1], top[b : b + 1], row))
    write_state(out_ref, memories, normals, totals, tops)


def weigh(entries, order, active):
    row = (1, LANES)
    since = jnp.zeros(row, f32)
    exponents = {}
    for j in order:
        _, total, top = entries[j]
        on = active(j)
        exponents[j] = jnp.where(on, top + since, FAR_BELOW)
        since = since + jnp.where(on, total, 0.0)
    highest = jnp.full(row, FAR_BELOW, f32)
    for j in order:
        highest = jnp.maximum(highest, exponents[j])
    weights = {
        j: jnp.where(active(j), jnp.exp(exponents[j] - highest), 0.0) for j in order
    }
    return weights, since, highest


def gathered(ref, entries, weights, d):
    memory = jnp.zeros((HEAD_DIM, LANES), f32)
    normal = jnp.zeros((1, LANES), f32)
    for j, w in weights.items():
        at = 0 if ref.shape[1] == HALF_ROWS else 64 * d
        memory = memory + w * ref[j, at : at + 64, :]
        normal = normal + w * entries[j][0]
    return memory, normal


def nearest_first(d, peers):
    return list(reversed(range(peers))) if d == 0 else list(range(peers))


def before(d, here):
    return (lambda j: j < here) if d == 0 else (lambda j: j > here)


def combine_kernel(here_ref, pieces_ref, out_ref, inside_ref, inside_tail_ref):
    peers = pieces_ref.shape[0]
    here = here_ref[0]
    memories, normals, totals, tops, tail = [], [], [], [], []
    for d in range(2):
        entries = [read_state(pieces_ref, j, d) for j in range(peers)]
        order = nearest_first(d, peers)
        weights, since, highest = weigh(entries, order, before(d, here))
        memory, normal = gathered(pieces_ref, entries, weights, d)
        inside_ref[64 * d : 64 * (d + 1), :] = memory
        tail += [normal, since, highest]
        weights, since, highest = weigh(entries, order, lambda j: j >= 0)
        memory, normal = gathered(pieces_ref, entries, weights, d)
        memories.append(memory)
        normals.append(normal)
        totals.append(since)
        tops.append(highest)
    inside_tail_ref[...] = packed_tail(tail)
    write_halves(out_ref, here_ref[1], memories, normals, totals, tops)


def head_sums(x, shape):
    first = iota(shape, 1) < HEAD_DIM
    a = jnp.sum(jnp.where(first, x, 0.0), axis=1, keepdims=True)
    b = jnp.sum(jnp.where(first, 0.0, x), axis=1, keepdims=True)
    return a, b


def mix_kernel(
    here_ref,
    pieces_ref,
    inside_ref,
    inside_tail_ref,
    query_ref,
    key_ref,
    value_ref,
    rate_ref,
    decay_ref,
    gain_ref,
    exit_ref,
    out_ref,
):
    peers = pieces_ref.shape[0]
    here = here_ref[0]
    length = query_ref.shape[0]
    wide = (length, LANES)
    query = query_ref[...]
    value = value_ref[...]
    query32 = query.astype(f32)
    rate = gate_rows(rate_ref)
    parts = three_parts(gate_rows(decay_ref))
    square = (length, length)
    row_at, lane_at = iota(square, 0), iota(square, 1)
    lane_head = iota((length, LANES), 1) // HEAD_DIM
    scores = []
    for h in range(2):
        own = jnp.where(lane_head == h, query32, 0.0).astype(bf16)
        scores.append(dot(own, key_ref[...], ((1,), (1,))) * HEAD_DIM ** (-0.5))
    summed = jnp.zeros(wide, f32)
    for d in range(2):
        entries = [read_state(pieces_ref, j, d) for j in range(peers)]
        weights, _, far_top = weigh(entries, nearest_first(d, peers), before(d, here))
        far_memory, far_normal = gathered(pieces_ref, entries, weights, d)
        near_normal = inside_tail_ref[3 * d : 3 * d + 1]
        near_total = inside_tail_ref[3 * d + 1 : 3 * d + 2]
        near_top = inside_tail_ref[3 * d + 2 : 3 * d + 3]
        lifted = near_total + far_top
        top_in = jnp.maximum(lifted, near_top)
        far_weight = jnp.exp(lifted - top_in)
        near_weight = jnp.exp(near_top - top_in)
        memory = far_weight * far_memory + near_weight * inside_ref[64 * d : 64 * (d + 1), :]
        normal = far_weight * far_normal + near_weight * near_normal

        seen = row_at >= lane_at if d == 0 else row_at <= lane_at
        seen_t = (row_at <= lane_at if d == 0 else row_at >= lane_at).astype(bf16)
        cumul_rows = dot_parts(parts, seen_t)
        cumul_cols = dot_parts([seen.astype(bf16)], parts[0], ((1,), (1,)))
        for part in parts[1:]:
            cumul_cols = cumul_cols + dot(seen.astype(bf16), part, ((1,), (1,)))

        first = iota((HEAD_DIM, LANES), 1) < HEAD_DIM
        block = jnp.concatenate(
            [jnp.where(first, memory, 0.0), jnp.where(first, 0.0, memory)], axis=0
        )
        carried_out = sum(dot(query, part) for part in three_parts(block))
        carried_den = head_sums(query32 * normal, wide)

        numer, denom, carry = [], [], []
        for h in range(2):
            r = 2 * d + h
            at_query = cumul_cols[:, r : r + 1]
            spread = at_query + (rate[r : r + 1] - cumul_rows[r : r + 1])
            spread = jnp.where(seen, spread, -jnp.inf)
            carried = at_query + top_in[:, HEAD_DIM * h : HEAD_DIM * h + 1]
            row_top = jnp.maximum(carried, jnp.max(spread, axis=1, keepdims=True))
            weighted = scores[h] * jnp.exp(spread - row_top)
            carry_weight = jnp.exp(carried - row_top)
            numer.append(dot_parts(three_parts(weighted), value))
            total = jnp.sum(weighted, axis=1, keepdims=True) + carry_weight * carried_den[h]
            denom.append(jnp.maximum(jnp.abs(total), jnp.exp(-row_top)))
            carry.append(carry_weight)
        top_part = by_head(numer[0], numer[1], wide)
        top_part = top_part + by_head(carry[0], carry[1], wide) * carried_out
        summed = summed + top_part / by_head(denom[0], denom[1], wide)
    squares = head_sums(summed * summed, wide)
    mean = by_head(squares[0], squares[1], wide) * (1.0 / HEAD_DIM)
    mixed = (summed * lax.rsqrt(mean + EPS) * gain_ref[...]).astype(bf16)
    out_ref[...] = dot(mixed, exit_ref[...]).astype(bf16)


def norm_kernel(pieces_ref, skip_ref, gain_ref, middle_ref, normed_ref):
    total = skip_ref[...].astype(f32)
    projected = pieces_ref[0].astype(f32)
    for j in range(1, pieces_ref.shape[0]):
        projected = projected + pieces_ref[j].astype(f32)
    middle = (total + projected).astype(bf16)
    middle_ref[...] = middle
    wide = middle.astype(f32)
    mean = jnp.mean(wide * wide, axis=1, keepdims=True)
    normed = (wide * lax.rsqrt(mean + EPS) * gain_ref[...]).astype(bf16)
    for copy in range(normed_ref.shape[0]):
        normed_ref[copy] = normed


def pack_kernel(up_ref, gate_ref, down_ref, out_ref):
    rest = HIDDEN - MAIN
    out_ref[:, :MAIN] = up_ref[:, :MAIN]
    tails = [up_ref[:, MAIN:].astype(f32), gate_ref[:, MAIN:].astype(f32)]
    out_ref[:, MAIN:GATE_AT] = jnp.concatenate(tails, axis=1).astype(bf16)
    out_ref[:, GATE_AT:DOWN_AT] = gate_ref[:, :MAIN]
    out_ref[:, DOWN_AT : DOWN_AT + MAIN] = down_ref[:, :MAIN]
    tails = [down_ref[:, MAIN:].astype(f32), jnp.zeros((out_ref.shape[0], rest), f32)]
    out_ref[:, DOWN_AT + MAIN :] = jnp.concatenate(tails, axis=1).astype(bf16)


def gated(inner, gate, taps):
    length = gate.shape[0]
    at = iota(gate.shape, 0)
    main = inner[:length]
    after_edge = inner[length : length + 1]
    before_edge = inner[length + 1 : length + 2]
    earlier = jnp.where(at == 0, before_edge, pltpu.roll(main, 1, 0))
    later = jnp.where(at == length - 1, after_edge, pltpu.roll(main, length - 1, 0))
    conv = taps[0:1] * earlier + taps[1:2] * main + taps[2:3] * later
    return jax.nn.gelu(conv) * gate


def feed_kernel(
    core_ref,
    tokens_ref,
    edges_ref,
    weight_ref,
    taps_ref,
    own_ref,
    other_ref,
    rows_ref,
    loaded_ref,
    hidden_ref,
    sems,
):
    length, width = tokens_ref.shape
    pairs, own, _ = own_ref.shape

    def keep(hidden, cols):
        for x in range(pairs):
            for c in range(2):
                slot = core_ref[0] if c == 0 else 1 - core_ref[0]
                at = pl.multiple_of(slot * (pairs * own) + x * own, own)
                row = (2 * x + c) * own
                hidden_ref[pl.ds(at, own), cols] = hidden[row : row + own].astype(bf16)

    step = width // FEED_STEPS
    copies = []
    for i in range(FEED_STEPS + 1):
        place = (pl.ds(i * step, step), pl.ds(0, DOWN_AT))
        if i == FEED_STEPS:
            place = (pl.ds(0, width), pl.ds(DOWN_AT, PACKED - DOWN_AT))
        copies.append(
            pltpu.make_async_copy(weight_ref.at[place], loaded_ref.at[place], sems.at[i])
        )
        copies[i].start()
    rows_ref[:length, :] = tokens_ref[...]
    rows_ref[length:, :] = edges_ref[...]
    inner, gate = None, None
    for i in range(FEED_STEPS):
        copies[i].wait()
        rows = slice(i * step, (i + 1) * step)
        left = rows_ref[:, rows]
        first = dot(left, loaded_ref[rows, :GATE_AT])
        second = dot(left[:length], loaded_ref[rows, GATE_AT:DOWN_AT])
        inner = first if inner is None else inner + first
        gate = second if gate is None else gate + second
    rounded = inner.astype(bf16).astype(f32)
    hidden = gated(rounded[:, :MAIN], gate, taps_ref[:, :MAIN])
    keep(hidden, slice(0, MAIN))
    gate = pltpu.roll(inner[:length, MAIN:], 64, 1)
    hidden = gated(rounded[:, MAIN:], gate, taps_ref[:, MAIN:])
    hidden = jnp.where(iota(hidden.shape, 1) < HIDDEN - MAIN, hidden, 0.0)
    keep(hidden, slice(MAIN, None))
    copies[FEED_STEPS].wait()
    for at in range(0, width, 256):
        cols = slice(at, at + 256)
        part = dot(hidden_ref[...], loaded_ref[cols, DOWN_AT:], ((1,), (1,))).astype(bf16)
        own_ref[:, :, cols] = part[: length // 2].reshape(pairs, own, 256)
        other_ref[:, :, cols] = part[length // 2 :].reshape(pairs, own, 256)


def near(x):
    return pltpu.with_memory_space_constraint(x, pltpu.VMEM)


def whole_call(kernel, out_shape, in_specs, name):
    def call(*args):
        return pl.pallas_call(
            kernel,
            out_shape=out_shape,
            in_specs=in_specs,
            out_specs=jax.tree.map(lambda _: VMEM, out_shape),
            name=name,
        )(*args)

    return call


def shape_of(dims, dtype):
    return jax.ShapeDtypeStruct(dims, dtype)


def exchanged(pieces, axis):
    return lax.all_to_all(pieces, axis, split_axis=0, concat_axis=0, tiled=True)


def body(
    lookup_request_vectors,
    lookup_address_vectors,
    lookup_content_vectors,
    admission_preactivation,
    retention_preactivation,
    extra_decay_terms,
    per_slot_rescale_factor,
    mixer_exit_matrix,
    skip_path_activity,
    mlp_rescale_factor,
    filter_widening_matrix,
    multiplier_widening_matrix,
    neighbour_filter_coefficients,
    contracting_matrix,
):
    length = lookup_request_vectors.shape[0]
    width = mixer_exit_matrix.shape[1]
    members = lax.axis_size(TP)

    packed = whole_call(
        pack_kernel, shape_of((filter_widening_matrix.shape[0], PACKED), bf16), [VMEM] * 3, "pack"
    )(filter_widening_matrix, multiplier_widening_matrix, contracting_matrix.T)
    weights = lax.all_gather(packed, SP, axis=0, tiled=True)

    decay = jax.nn.log_sigmoid(retention_preactivation) + extra_decay_terms
    rate = admission_preactivation

    state = pltpu.VMEM((8, STATE_ROWS, LANES), f32)
    summary = whole_call(summarize_kernel, state, [VMEM] * 4, "summarize")(
        lookup_address_vectors, lookup_content_vectors, rate, decay
    )
    pieces = near(exchanged(summary, "sp_1"))
    along, inside, inside_tail = whole_call(
        combine_kernel,
        (
            pltpu.VMEM((8, HALF_ROWS, LANES), f32),
            pltpu.VMEM((128, LANES), f32),
            pltpu.VMEM((8, LANES), f32),
        ),
        [SMEM, VMEM],
        "combine",
    )(jnp.stack([lax.axis_index("sp_1"), lax.axis_index("sp_0")]), pieces)
    pieces = near(exchanged(along, "sp_0"))
    partial_out = whole_call(
        mix_kernel, pltpu.VMEM((length, width), bf16), [SMEM] + [VMEM] * 10, "mix"
    )(
        lax.axis_index("sp_0").reshape(1),
        pieces,
        near(inside),
        near(inside_tail),
        lookup_request_vectors,
        lookup_address_vectors,
        lookup_content_vectors,
        rate,
        decay,
        per_slot_rescale_factor.reshape(1, LANES),
        mixer_exit_matrix,
    )
    own = length // members
    pieces = near(exchanged(partial_out.reshape(members, own, width), TP))
    middle, normed = whole_call(
        norm_kernel,
        (shape_of((own, width), bf16), pltpu.VMEM((members, own, width), bf16)),
        [VMEM] * 3,
        "norm",
    )(pieces, skip_path_activity, mlp_rescale_factor.reshape(1, width))
    tokens = exchanged(normed, TP).reshape(length, width)

    peers = lax.axis_size(SP)
    up = [(i, i + 1) for i in range(peers - 1)]
    down = [(j, i) for i, j in up]
    earlier = lax.ppermute(tokens[length - 1 :], SP, up)
    later = lax.ppermute(tokens[:1], SP, down)
    edges = jnp.concatenate([later, earlier, jnp.zeros((14, width), bf16)], axis=0)

    halves = pltpu.VMEM((members // 2, own, width), bf16)
    own_half, other_half = pl.pallas_call(
        feed_kernel,
        out_shape=(halves, halves),
        in_specs=[SMEM, VMEM, VMEM, ANY, VMEM],
        out_specs=(VMEM, VMEM),
        scratch_shapes=[
            pltpu.VMEM((length + 16, width), bf16),
            pltpu.VMEM((width, PACKED), bf16),
            pltpu.VMEM((length, 768), bf16),
            pltpu.SemaphoreType.DMA((FEED_STEPS + 1,)),
        ],
        name="feed",
    )(
        lax.axis_index("core").reshape(1),
        near(tokens),
        near(edges),
        pltpu.with_memory_space_constraint(weights, pltpu.HBM),
        jnp.pad(neighbour_filter_coefficients, ((0, 0), (0, 768 - HIDDEN))),
    )
    from_partner = lax.ppermute(other_half, "core", [(0, 1), (1, 0)])
    pair = (own_half.astype(f32) + from_partner.astype(f32)).astype(bf16)
    pieces = exchanged(pair, "x").astype(f32)
    total = middle.astype(f32)
    for j in range(pieces.shape[0]):
        total = total + pieces[j]
    return total.astype(bf16)


def solution(mesh):
    split = Mesh(mesh.devices.reshape(8, 8, 4, 2), SP_TP)
    placed = (
        P(SP, TP),
        P(SP, TP),
        P(SP, TP),
        P(None, TP, SP),
        P(None, TP, SP),
        P(None, TP, SP),
        P(TP),
        P(TP, None),
        P(SP_TP, None),
        P(),
        P(SP, TP),
        P(SP, TP),
        P(None, TP),
        P(TP, SP),
    )
    return jax.shard_map(
        body, mesh=split, in_specs=placed, out_specs=P(SP_TP, None), check_vma=False
    )
```

```python
import jax
import jax.numpy as jnp
from jax import lax
from jax.experimental import pallas as pl
from jax.experimental.pallas import tpu as pltpu
from jax.sharding import Mesh
from jax.sharding import PartitionSpec as P

HEAD_DIM = 64
SP = ("sp_0", "sp_1")
TP = ("x", "core")
SP_TP = SP + TP
EPS = 1e-06
FAR_BELOW = -1e30
LANES = 128
HIDDEN = 704
MAIN = 640
GATE_AT = MAIN + 128
DOWN_AT = GATE_AT + MAIN
PACKED = DOWN_AT + 768
FEED_STEPS = 4
ANY = pl.BlockSpec(memory_space=pl.ANY)
f32 = jnp.float32
bf16 = jnp.bfloat16
VMEM = pl.BlockSpec(memory_space=pltpu.VMEM)
SMEM = pl.BlockSpec(memory_space=pltpu.SMEM)


def three_parts(x):
    hi = x.astype(bf16)
    rest = x - hi.astype(f32)
    mid = rest.astype(bf16)
    low = (rest - mid.astype(f32)).astype(bf16)
    return hi, mid, low


def dot(a, b, dims=((1,), (0,))):
    return lax.dot_general(a, b, (dims, ((), ())), preferred_element_type=f32)


def dot_parts(parts, b, dims=((1,), (0,))):
    total = dot(parts[0], b, dims)
    for part in parts[1:]:
        total = total + dot(part, b, dims)
    return total


def iota(shape, dim):
    return lax.broadcasted_iota(jnp.int32, shape, dim)


def gate_rows(ref):
    place = iota((8, ref.shape[2]), 0)
    out = jnp.zeros((8, ref.shape[2]), f32)
    for d in range(2):
        for h in range(2):
            out = jnp.where(place == 2 * d + h, ref[d, h : h + 1, :], out)
    return out


def by_head(first, second, shape):
    return jnp.where(iota(shape, len(shape) - 1) < HEAD_DIM, first, second)


def packed_rows(rows, count):
    place = iota((count, LANES), 0)
    out = jnp.zeros((count, LANES), f32)
    for k, row in enumerate(rows):
        out = jnp.where(place == k, row, out)
    return out


def nothing(rows):
    line = jnp.zeros((1, LANES), f32)
    return line, jnp.zeros((rows, LANES), f32), line, jnp.full((1, LANES), FAR_BELOW, f32)


def combined(earlier, later):
    total_a, memory_a, normal_a, top_a = earlier
    total_b, memory_b, normal_b, top_b = later
    lifted = total_b + top_a
    top = jnp.maximum(lifted, top_b)
    weight_a, weight_b = jnp.exp(lifted - top), jnp.exp(top_b - top)
    memory = weight_a * memory_a + weight_b * memory_b
    return total_a + total_b, memory, weight_a * normal_a + weight_b * normal_b, top


def in_order(d, peers):
    return range(peers) if d == 0 else reversed(range(peers))


def summarize_kernel(key_ref, value_ref, rate_ref, decay_ref, out_ref):
    length = key_ref.shape[0]
    rate = gate_rows(rate_ref)
    decay = gate_rows(decay_ref)
    upper = (iota((length, length), 0) <= iota((length, length), 1)).astype(bf16)
    cumul = dot_parts(three_parts(decay), upper)
    total = cumul[:, length - 1 : length]
    is_forward = iota((8, length), 0) < 2
    weight = jnp.where(is_forward, total - cumul, cumul - decay) + rate
    top = jnp.max(weight, axis=1, keepdims=True)
    fresh = jnp.exp(weight - top)
    key_t = key_ref[...].astype(f32).T * HEAD_DIM ** (-0.5)
    value = value_ref[...]
    normal_all = dot_parts(three_parts(fresh), key_ref[...]) * HEAD_DIM ** (-0.5)
    memories, normals, totals, tops = [], [], [], []
    for d in range(2):
        a, b = 2 * d, 2 * d + 1
        spread = jnp.concatenate(
            [
                jnp.broadcast_to(fresh[a : a + 1], (HEAD_DIM, length)),
                jnp.broadcast_to(fresh[b : b + 1], (HEAD_DIM, length)),
            ],
            axis=0,
        )
        both = dot_parts(three_parts(key_t * spread), value)
        memories.append(by_head(both[:HEAD_DIM], both[HEAD_DIM:], (HEAD_DIM, LANES)))
        row = (1, LANES)
        normals.append(by_head(normal_all[a : a + 1], normal_all[b : b + 1], row))
        totals.append(by_head(total[a : a + 1], total[b : b + 1], row))
        tops.append(by_head(top[a : a + 1], top[b : b + 1], row))
    tail = packed_rows([*normals, *totals, *tops], 8)
    for j in range(out_ref.shape[0]):
        part = [memory[8 * j : 8 * (j + 1)] for memory in memories]
        out_ref[j, :16, :] = jnp.concatenate(part, axis=0)
        out_ref[j, 16:, :] = tail


def along_kernel(here_ref, pieces_ref, out_ref, inside_ref):
    peers = pieces_ref.shape[0]
    tails = [pieces_ref[j, 16:, :] for j in range(peers)]
    memories = [pieces_ref[j, :16, :] for j in range(peers)]
    reaching = []
    wholes = []
    for d in range(2):
        state = nothing(8)
        reached = {}
        for j in in_order(d, peers):
            reached[j] = state
            normal, total, top = (tails[j][d + k : d + k + 1] for k in (0, 2, 4))
            state = combined(state, (total, memories[j][8 * d : 8 * (d + 1)], normal, top))
        reaching.append(reached)
        total, memory, normal, top = state
        rows = packed_rows([normal, total, top], 8)
        wholes.append(jnp.concatenate([memory, rows], axis=0))
    for j in range(peers):
        lines = []
        for d in range(2):
            total, memory, normal, top = reaching[d][j]
            inside_ref[j, 8 * d : 8 * (d + 1), :] = memory
            lines += [total, normal, top]
        inside_ref[j, 16:, :] = packed_rows(lines, 8)
    for j in range(out_ref.shape[0]):
        out_ref[j] = jnp.where(j > here_ref[0], wholes[0], wholes[1])


def across_kernel(here_ref, pieces_ref, inside_ref, out_ref):
    peers = pieces_ref.shape[0]
    here = here_ref[0]
    far = []
    for d in range(2):
        state = nothing(8)
        for j in in_order(d, peers):
            piece = pieces_ref[j]
            later = (piece[9:10], piece[:8], piece[8:9], piece[10:11])
            on = j < here if d == 0 else j > here
            state = [jnp.where(on, x, y) for x, y in zip(combined(state, later), state)]
        far.append(state)
    for j in range(out_ref.shape[0]):
        memories, normals, tops = [], [], []
        lines = inside_ref[j, 16:, :]
        for d in range(2):
            total, normal, top = (lines[3 * d + k : 3 * d + k + 1] for k in range(3))
            near_state = (total, inside_ref[j, 8 * d : 8 * (d + 1), :], normal, top)
            _, memory, normal, top = combined(far[d], near_state)
            memories.append(memory)
            normals.append(normal)
            tops.append(top)
        out_ref[j, :16, :] = jnp.concatenate(memories, axis=0)
        out_ref[j, 16:, :] = packed_rows(normals + tops, 8)


def head_sums(x, shape):
    first = iota(shape, 1) < HEAD_DIM
    a = jnp.sum(jnp.where(first, x, 0.0), axis=1, keepdims=True)
    b = jnp.sum(jnp.where(first, 0.0, x), axis=1, keepdims=True)
    return a, b


def mix_kernel(
    pieces_ref,
    query_ref,
    key_ref,
    value_ref,
    rate_ref,
    decay_ref,
    gain_ref,
    exit_ref,
    out_ref,
):
    peers = pieces_ref.shape[0]
    tail = pieces_ref[0, 16:, :]
    length = query_ref.shape[0]
    wide = (length, LANES)
    query = query_ref[...]
    value = value_ref[...]
    query32 = query.astype(f32)
    rate = gate_rows(rate_ref)
    parts = three_parts(gate_rows(decay_ref))
    square = (length, length)
    row_at, lane_at = iota(square, 0), iota(square, 1)
    lane_head = iota((length, LANES), 1) // HEAD_DIM
    scores = []
    for h in range(2):
        own = jnp.where(lane_head == h, query32, 0.0).astype(bf16)
        scores.append(dot(own, key_ref[...], ((1,), (1,))) * HEAD_DIM ** (-0.5))
    summed = jnp.zeros(wide, f32)
    for d in range(2):
        memory = jnp.concatenate(
            [pieces_ref[j, 8 * d : 8 * (d + 1), :] for j in range(peers)], axis=0
        )
        normal, top_in = tail[d : d + 1], tail[2 + d : 3 + d]

        seen = row_at >= lane_at if d == 0 else row_at <= lane_at
        seen_t = (row_at <= lane_at if d == 0 else row_at >= lane_at).astype(bf16)
        cumul_rows = dot_parts(parts, seen_t)
        cumul_cols = dot_parts([seen.astype(bf16)], parts[0], ((1,), (1,)))
        for part in parts[1:]:
            cumul_cols = cumul_cols + dot(seen.astype(bf16), part, ((1,), (1,)))

        first = iota((HEAD_DIM, LANES), 1) < HEAD_DIM
        block = jnp.concatenate(
            [jnp.where(first, memory, 0.0), jnp.where(first, 0.0, memory)], axis=0
        )
        carried_out = sum(dot(query, part) for part in three_parts(block))
        carried_den = head_sums(query32 * normal, wide)

        numer, denom, carry = [], [], []
        for h in range(2):
            r = 2 * d + h
            at_query = cumul_cols[:, r : r + 1]
            spread = at_query + (rate[r : r + 1] - cumul_rows[r : r + 1])
            spread = jnp.where(seen, spread, -jnp.inf)
            carried = at_query + top_in[:, HEAD_DIM * h : HEAD_DIM * h + 1]
            row_top = jnp.maximum(carried, jnp.max(spread, axis=1, keepdims=True))
            weighted = scores[h] * jnp.exp(spread - row_top)
            carry_weight = jnp.exp(carried - row_top)
            numer.append(dot_parts(three_parts(weighted), value))
            total = jnp.sum(weighted, axis=1, keepdims=True) + carry_weight * carried_den[h]
            denom.append(jnp.maximum(jnp.abs(total), jnp.exp(-row_top)))
            carry.append(carry_weight)
        top_part = by_head(numer[0], numer[1], wide)
        top_part = top_part + by_head(carry[0], carry[1], wide) * carried_out
        summed = summed + top_part / by_head(denom[0], denom[1], wide)
    squares = head_sums(summed * summed, wide)
    mean = by_head(squares[0], squares[1], wide) * (1.0 / HEAD_DIM)
    mixed = (summed * lax.rsqrt(mean + EPS) * gain_ref[...]).astype(bf16)
    out_ref[...] = dot(mixed, exit_ref[...]).astype(bf16)


def norm_kernel(pieces_ref, skip_ref, gain_ref, middle_ref, normed_ref):
    total = skip_ref[...].astype(f32)
    projected = pieces_ref[0].astype(f32)
    for j in range(1, pieces_ref.shape[0]):
        projected = projected + pieces_ref[j].astype(f32)
    middle = (total + projected).astype(bf16)
    middle_ref[...] = middle
    wide = middle.astype(f32)
    mean = jnp.mean(wide * wide, axis=1, keepdims=True)
    normed = (wide * lax.rsqrt(mean + EPS) * gain_ref[...]).astype(bf16)
    for copy in range(normed_ref.shape[0]):
        normed_ref[copy] = normed


def pack_kernel(up_ref, gate_ref, down_ref, out_ref):
    rest = HIDDEN - MAIN
    out_ref[:, :MAIN] = up_ref[:, :MAIN]
    tails = [up_ref[:, MAIN:].astype(f32), gate_ref[:, MAIN:].astype(f32)]
    out_ref[:, MAIN:GATE_AT] = jnp.concatenate(tails, axis=1).astype(bf16)
    out_ref[:, GATE_AT:DOWN_AT] = gate_ref[:, :MAIN]
    out_ref[:, DOWN_AT : DOWN_AT + MAIN] = down_ref[:, :MAIN]
    tails = [down_ref[:, MAIN:].astype(f32), jnp.zeros((out_ref.shape[0], rest), f32)]
    out_ref[:, DOWN_AT + MAIN :] = jnp.concatenate(tails, axis=1).astype(bf16)


def gated(inner, gate, taps):
    length = gate.shape[0]
    at = iota(gate.shape, 0)
    main = inner[:length]
    after_edge = inner[length : length + 1]
    before_edge = inner[length + 1 : length + 2]
    earlier = jnp.where(at == 0, before_edge, pltpu.roll(main, 1, 0))
    later = jnp.where(at == length - 1, after_edge, pltpu.roll(main, length - 1, 0))
    conv = taps[0:1] * earlier + taps[1:2] * main + taps[2:3] * later
    return jax.nn.gelu(conv) * gate


def feed_kernel(
    core_ref,
    tokens_ref,
    edges_ref,
    weight_ref,
    taps_ref,
    own_ref,
    other_ref,
    rows_ref,
    loaded_ref,
    hidden_ref,
    sems,
):
    length, width = tokens_ref.shape
    pairs, own, _ = own_ref.shape

    def keep(hidden, cols):
        for x in range(pairs):
            for c in range(2):
                slot = core_ref[0] if c == 0 else 1 - core_ref[0]
                at = pl.multiple_of(slot * (pairs * own) + x * own, own)
                row = (2 * x + c) * own
                hidden_ref[pl.ds(at, own), cols] = hidden[row : row + own].astype(bf16)

    step = width // FEED_STEPS
    copies = []
    for i in range(FEED_STEPS + 1):
        place = (pl.ds(i * step, step), pl.ds(0, DOWN_AT))
        if i == FEED_STEPS:
            place = (pl.ds(0, width), pl.ds(DOWN_AT, PACKED - DOWN_AT))
        copies.append(
            pltpu.make_async_copy(weight_ref.at[place], loaded_ref.at[place], sems.at[i])
        )
        copies[i].start()
    rows_ref[:length, :] = tokens_ref[...]
    rows_ref[length:, :] = edges_ref[...]
    inner, gate = None, None
    for i in range(FEED_STEPS):
        copies[i].wait()
        rows = slice(i * step, (i + 1) * step)
        left = rows_ref[:, rows]
        first = dot(left, loaded_ref[rows, :GATE_AT])
        second = dot(left[:length], loaded_ref[rows, GATE_AT:DOWN_AT])
        inner = first if inner is None else inner + first
        gate = second if gate is None else gate + second
    rounded = inner.astype(bf16).astype(f32)
    hidden = gated(rounded[:, :MAIN], gate, taps_ref[:, :MAIN])
    keep(hidden, slice(0, MAIN))
    gate = pltpu.roll(inner[:length, MAIN:], 64, 1)
    hidden = gated(rounded[:, MAIN:], gate, taps_ref[:, MAIN:])
    hidden = jnp.where(iota(hidden.shape, 1) < HIDDEN - MAIN, hidden, 0.0)
    keep(hidden, slice(MAIN, None))
    copies[FEED_STEPS].wait()
    for at in range(0, width, 256):
        cols = slice(at, at + 256)
        part = dot(hidden_ref[...], loaded_ref[cols, DOWN_AT:], ((1,), (1,))).astype(bf16)
        own_ref[:, :, cols] = part[: length // 2].reshape(pairs, own, 256)
        other_ref[:, :, cols] = part[length // 2 :].reshape(pairs, own, 256)


def near(x):
    return pltpu.with_memory_space_constraint(x, pltpu.VMEM)


def whole_call(kernel, out_shape, in_specs, name):
    def call(*args):
        return pl.pallas_call(
            kernel,
            out_shape=out_shape,
            in_specs=in_specs,
            out_specs=jax.tree.map(lambda _: VMEM, out_shape),
            name=name,
        )(*args)

    return call


def shape_of(dims, dtype):
    return jax.ShapeDtypeStruct(dims, dtype)


def exchanged(pieces, axis):
    return lax.all_to_all(pieces, axis, split_axis=0, concat_axis=0, tiled=True)


def body(
    lookup_request_vectors,
    lookup_address_vectors,
    lookup_content_vectors,
    admission_preactivation,
    retention_preactivation,
    extra_decay_terms,
    per_slot_rescale_factor,
    mixer_exit_matrix,
    skip_path_activity,
    mlp_rescale_factor,
    filter_widening_matrix,
    multiplier_widening_matrix,
    neighbour_filter_coefficients,
    contracting_matrix,
):
    length = lookup_request_vectors.shape[0]
    width = mixer_exit_matrix.shape[1]
    members = lax.axis_size(TP)

    packed = whole_call(
        pack_kernel, shape_of((filter_widening_matrix.shape[0], PACKED), bf16), [VMEM] * 3, "pack"
    )(filter_widening_matrix, multiplier_widening_matrix, contracting_matrix.T)
    weights = lax.all_gather(packed, SP, axis=0, tiled=True)

    decay = jax.nn.log_sigmoid(retention_preactivation) + extra_decay_terms
    rate = admission_preactivation

    row, column = lax.axis_index("sp_0").reshape(1), "sp_1"
    pieces = pltpu.VMEM((8, 24, LANES), f32)
    summary = whole_call(summarize_kernel, pieces, [VMEM] * 4, "summarize")(
        lookup_address_vectors, lookup_content_vectors, rate, decay
    )
    along, inside = whole_call(
        along_kernel,
        (pltpu.VMEM((8, 16, LANES), f32), pltpu.VMEM((8, 24, LANES), f32)),
        [SMEM, VMEM],
        "along",
    )(row, near(exchanged(summary, column)))
    across = whole_call(across_kernel, pieces, [SMEM, VMEM, VMEM], "across")(
        row, near(exchanged(along, "sp_0")), near(inside)
    )
    partial_out = whole_call(
        mix_kernel, pltpu.VMEM((length, width), bf16), [VMEM] * 8, "mix"
    )(
        near(exchanged(across, column)),
        lookup_request_vectors,
        lookup_address_vectors,
        lookup_content_vectors,
        rate,
        decay,
        per_slot_rescale_factor.reshape(1, LANES),
        mixer_exit_matrix,
    )
    own = length // members
    pieces = near(exchanged(partial_out.reshape(members, own, width), TP))
    middle, normed = whole_call(
        norm_kernel,
        (shape_of((own, width), bf16), pltpu.VMEM((members, own, width), bf16)),
        [VMEM] * 3,
        "norm",
    )(pieces, skip_path_activity, mlp_rescale_factor.reshape(1, width))
    tokens = exchanged(normed, TP).reshape(length, width)

    peers = lax.axis_size(SP)
    up = [(i, i + 1) for i in range(peers - 1)]
    down = [(j, i) for i, j in up]
    earlier = lax.ppermute(tokens[length - 1 :], SP, up)
    later = lax.ppermute(tokens[:1], SP, down)
    edges = jnp.concatenate([later, earlier, jnp.zeros((14, width), bf16)], axis=0)

    halves = pltpu.VMEM((members // 2, own, width), bf16)
    own_half, other_half = pl.pallas_call(
        feed_kernel,
        out_shape=(halves, halves),
        in_specs=[SMEM, VMEM, VMEM, ANY, VMEM],
        out_specs=(VMEM, VMEM),
        scratch_shapes=[
            pltpu.VMEM((length + 16, width), bf16),
            pltpu.VMEM((width, PACKED), bf16),
            pltpu.VMEM((length, 768), bf16),
            pltpu.SemaphoreType.DMA((FEED_STEPS + 1,)),
        ],
        name="feed",
    )(
        lax.axis_index("core").reshape(1),
        near(tokens),
        near(edges),
        pltpu.with_memory_space_constraint(weights, pltpu.HBM),
        jnp.pad(neighbour_filter_coefficients, ((0, 0), (0, 768 - HIDDEN))),
    )
    from_partner = lax.ppermute(other_half, "core", [(0, 1), (1, 0)])
    pair = (own_half.astype(f32) + from_partner.astype(f32)).astype(bf16)
    pieces = exchanged(pair, "x").astype(f32)
    total = middle.astype(f32)
    for j in range(pieces.shape[0]):
        total = total + pieces[j]
    return total.astype(bf16)


def solution(mesh):
    split = Mesh(mesh.devices.reshape(8, 8, 4, 2), SP_TP)
    placed = (
        P(SP, TP),
        P(SP, TP),
        P(SP, TP),
        P(None, TP, SP),
        P(None, TP, SP),
        P(None, TP, SP),
        P(TP),
        P(TP, None),
        P(SP_TP, None),
        P(),
        P(SP, TP),
        P(SP, TP),
        P(None, TP),
        P(TP, SP),
    )
    return jax.shard_map(
        body, mesh=split, in_specs=placed, out_specs=P(SP_TP, None), check_vma=False
    )
```

```python
import jax
import jax.numpy as jnp
from jax import lax
from jax.experimental import pallas as pl
from jax.experimental.pallas import tpu as pltpu
from jax.sharding import Mesh
from jax.sharding import PartitionSpec as P

HEAD_DIM = 64
SP = ("sp_0", "sp_1")
TP = ("x", "core")
SP_TP = SP + TP
EPS = 1e-06
FAR_BELOW = -1e30
LANES = 128
HIDDEN = 704
MAIN = 640
GATE_AT = MAIN + 128
DOWN_AT = GATE_AT + MAIN
PACKED = DOWN_AT + 768
FEED_STEPS = 2
FEED_COLS = 256
ANY = pl.BlockSpec(memory_space=pl.ANY)
f32 = jnp.float32
bf16 = jnp.bfloat16
VMEM = pl.BlockSpec(memory_space=pltpu.VMEM)
SMEM = pl.BlockSpec(memory_space=pltpu.SMEM)


def three_parts(x):
    hi = x.astype(bf16)
    rest = x - hi.astype(f32)
    mid = rest.astype(bf16)
    low = (rest - mid.astype(f32)).astype(bf16)
    return hi, mid, low


def dot(a, b, dims=((1,), (0,))):
    return lax.dot_general(a, b, (dims, ((), ())), preferred_element_type=f32)


def dot_parts(parts, b, dims=((1,), (0,))):
    total = dot(parts[0], b, dims)
    for part in parts[1:]:
        total = total + dot(part, b, dims)
    return total


def iota(shape, dim):
    return lax.broadcasted_iota(jnp.int32, shape, dim)


def gate_rows(ref):
    place = iota((8, ref.shape[2]), 0)
    out = jnp.zeros((8, ref.shape[2]), f32)
    for d in range(2):
        for h in range(2):
            out = jnp.where(place == 2 * d + h, ref[d, h : h + 1, :], out)
    return out


def by_head(first, second, shape):
    return jnp.where(iota(shape, len(shape) - 1) < HEAD_DIM, first, second)


def packed_rows(rows, count):
    place = iota((count, LANES), 0)
    out = jnp.zeros((count, LANES), f32)
    for k, row in enumerate(rows):
        out = jnp.where(place == k, row, out)
    return out


def nothing(rows):
    line = jnp.zeros((1, LANES), f32)
    return line, jnp.zeros((rows, LANES), f32), line, jnp.full((1, LANES), FAR_BELOW, f32)


def combined(earlier, later):
    total_a, memory_a, normal_a, top_a = earlier
    total_b, memory_b, normal_b, top_b = later
    lifted = total_b + top_a
    top = jnp.maximum(lifted, top_b)
    weight_a, weight_b = jnp.exp(lifted - top), jnp.exp(top_b - top)
    memory = weight_a * memory_a + weight_b * memory_b
    return total_a + total_b, memory, weight_a * normal_a + weight_b * normal_b, top


def in_order(d, peers):
    return range(peers) if d == 0 else reversed(range(peers))


def summarize_kernel(key_ref, value_ref, rate_ref, decay_ref, out_ref):
    length = key_ref.shape[0]
    rate = gate_rows(rate_ref)
    decay = gate_rows(decay_ref)
    upper = (iota((length, length), 0) <= iota((length, length), 1)).astype(bf16)
    cumul = dot_parts(three_parts(decay), upper)
    total = cumul[:, length - 1 : length]
    is_forward = iota((8, length), 0) < 2
    weight = jnp.where(is_forward, total - cumul, cumul - decay) + rate
    top = jnp.max(weight, axis=1, keepdims=True)
    fresh = jnp.exp(weight - top)
    key_t = key_ref[...].astype(f32).T * HEAD_DIM ** (-0.5)
    value = value_ref[...]
    normal_all = dot_parts(three_parts(fresh), key_ref[...]) * HEAD_DIM ** (-0.5)
    memories, normals, totals, tops = [], [], [], []
    for d in range(2):
        a, b = 2 * d, 2 * d + 1
        spread = jnp.concatenate(
            [
                jnp.broadcast_to(fresh[a : a + 1], (HEAD_DIM, length)),
                jnp.broadcast_to(fresh[b : b + 1], (HEAD_DIM, length)),
            ],
            axis=0,
        )
        both = dot_parts(three_parts(key_t * spread), value)
        memories.append(by_head(both[:HEAD_DIM], both[HEAD_DIM:], (HEAD_DIM, LANES)))
        row = (1, LANES)
        normals.append(by_head(normal_all[a : a + 1], normal_all[b : b + 1], row))
        totals.append(by_head(total[a : a + 1], total[b : b + 1], row))
        tops.append(by_head(top[a : a + 1], top[b : b + 1], row))
    tail = packed_rows([*normals, *totals, *tops], 8)
    for j in range(out_ref.shape[0]):
        part = [memory[8 * j : 8 * (j + 1)] for memory in memories]
        out_ref[j, :16, :] = jnp.concatenate(part, axis=0)
        out_ref[j, 16:, :] = tail


def along_kernel(here_ref, pieces_ref, out_ref, inside_ref):
    peers = pieces_ref.shape[0]
    tails = [pieces_ref[j, 16:, :] for j in range(peers)]
    memories = [pieces_ref[j, :16, :] for j in range(peers)]
    reaching = []
    wholes = []
    for d in range(2):
        state = nothing(8)
        reached = {}
        for j in in_order(d, peers):
            reached[j] = state
            normal, total, top = (tails[j][d + k : d + k + 1] for k in (0, 2, 4))
            state = combined(state, (total, memories[j][8 * d : 8 * (d + 1)], normal, top))
        reaching.append(reached)
        total, memory, normal, top = state
        rows = packed_rows([normal, total, top], 8)
        wholes.append(jnp.concatenate([memory, rows], axis=0))
    for j in range(peers):
        lines = []
        for d in range(2):
            total, memory, normal, top = reaching[d][j]
            inside_ref[j, 8 * d : 8 * (d + 1), :] = memory
            lines += [total, normal, top]
        inside_ref[j, 16:, :] = packed_rows(lines, 8)
    for j in range(out_ref.shape[0]):
        out_ref[j] = jnp.where(j > here_ref[0], wholes[0], wholes[1])


def across_kernel(here_ref, pieces_ref, inside_ref, out_ref):
    peers = pieces_ref.shape[0]
    here = here_ref[0]
    far = []
    for d in range(2):
        state = nothing(8)
        for j in in_order(d, peers):
            piece = pieces_ref[j]
            later = (piece[9:10], piece[:8], piece[8:9], piece[10:11])
            on = j < here if d == 0 else j > here
            state = [jnp.where(on, x, y) for x, y in zip(combined(state, later), state)]
        far.append(state)
    for j in range(out_ref.shape[0]):
        memories, normals, tops = [], [], []
        lines = inside_ref[j, 16:, :]
        for d in range(2):
            total, normal, top = (lines[3 * d + k : 3 * d + k + 1] for k in range(3))
            near_state = (total, inside_ref[j, 8 * d : 8 * (d + 1), :], normal, top)
            _, memory, normal, top = combined(far[d], near_state)
            memories.append(memory)
            normals.append(normal)
            tops.append(top)
        out_ref[j, :16, :] = jnp.concatenate(memories, axis=0)
        out_ref[j, 16:, :] = packed_rows(normals + tops, 8)


def head_sums(x, shape):
    first = iota(shape, 1) < HEAD_DIM
    a = jnp.sum(jnp.where(first, x, 0.0), axis=1, keepdims=True)
    b = jnp.sum(jnp.where(first, 0.0, x), axis=1, keepdims=True)
    return a, b


def mix_kernel(
    pieces_ref,
    query_ref,
    key_ref,
    value_ref,
    rate_ref,
    decay_ref,
    gain_ref,
    exit_ref,
    out_ref,
):
    peers = pieces_ref.shape[0]
    tail = pieces_ref[0, 16:, :]
    length = query_ref.shape[0]
    wide = (length, LANES)
    query = query_ref[...]
    value = value_ref[...]
    query32 = query.astype(f32)
    rate = gate_rows(rate_ref)
    parts = three_parts(gate_rows(decay_ref))
    square = (length, length)
    row_at, lane_at = iota(square, 0), iota(square, 1)
    lane_head = iota((length, LANES), 1) // HEAD_DIM
    scores = []
    for h in range(2):
        own = jnp.where(lane_head == h, query32, 0.0).astype(bf16)
        scores.append(dot(own, key_ref[...], ((1,), (1,))) * HEAD_DIM ** (-0.5))
    summed = jnp.zeros(wide, f32)
    for d in range(2):
        memory = jnp.concatenate(
            [pieces_ref[j, 8 * d : 8 * (d + 1), :] for j in range(peers)], axis=0
        )
        normal, top_in = tail[d : d + 1], tail[2 + d : 3 + d]

        seen = row_at >= lane_at if d == 0 else row_at <= lane_at
        seen_t = (row_at <= lane_at if d == 0 else row_at >= lane_at).astype(bf16)
        cumul_rows = dot_parts(parts, seen_t)
        cumul_cols = dot_parts([seen.astype(bf16)], parts[0], ((1,), (1,)))
        for part in parts[1:]:
            cumul_cols = cumul_cols + dot(seen.astype(bf16), part, ((1,), (1,)))

        first = iota((HEAD_DIM, LANES), 1) < HEAD_DIM
        block = jnp.concatenate(
            [jnp.where(first, memory, 0.0), jnp.where(first, 0.0, memory)], axis=0
        )
        carried_out = sum(dot(query, part) for part in three_parts(block))
        carried_den = head_sums(query32 * normal, wide)

        numer, denom, carry = [], [], []
        for h in range(2):
            r = 2 * d + h
            at_query = cumul_cols[:, r : r + 1]
            spread = at_query + (rate[r : r + 1] - cumul_rows[r : r + 1])
            spread = jnp.where(seen, spread, -jnp.inf)
            carried = at_query + top_in[:, HEAD_DIM * h : HEAD_DIM * h + 1]
            row_top = jnp.maximum(carried, jnp.max(spread, axis=1, keepdims=True))
            weighted = scores[h] * jnp.exp(spread - row_top)
            carry_weight = jnp.exp(carried - row_top)
            numer.append(dot_parts(three_parts(weighted), value))
            total = jnp.sum(weighted, axis=1, keepdims=True) + carry_weight * carried_den[h]
            denom.append(jnp.maximum(jnp.abs(total), jnp.exp(-row_top)))
            carry.append(carry_weight)
        top_part = by_head(numer[0], numer[1], wide)
        top_part = top_part + by_head(carry[0], carry[1], wide) * carried_out
        summed = summed + top_part / by_head(denom[0], denom[1], wide)
    squares = head_sums(summed * summed, wide)
    mean = by_head(squares[0], squares[1], wide) * (1.0 / HEAD_DIM)
    mixed = (summed * lax.rsqrt(mean + EPS) * gain_ref[...]).astype(bf16)
    out_ref[...] = dot(mixed, exit_ref[...]).astype(bf16)


def norm_kernel(pieces_ref, skip_ref, gain_ref, middle_ref, normed_ref):
    total = skip_ref[...].astype(f32)
    projected = pieces_ref[0].astype(f32)
    for j in range(1, pieces_ref.shape[0]):
        projected = projected + pieces_ref[j].astype(f32)
    middle = (total + projected).astype(bf16)
    middle_ref[...] = middle
    wide = middle.astype(f32)
    mean = jnp.mean(wide * wide, axis=1, keepdims=True)
    normed = (wide * lax.rsqrt(mean + EPS) * gain_ref[...]).astype(bf16)
    for copy in range(normed_ref.shape[0]):
        normed_ref[copy] = normed


def pack_kernel(up_ref, gate_ref, down_ref, out_ref):
    rest = HIDDEN - MAIN
    out_ref[:, :MAIN] = up_ref[:, :MAIN]
    tails = [up_ref[:, MAIN:].astype(f32), gate_ref[:, MAIN:].astype(f32)]
    out_ref[:, MAIN:GATE_AT] = jnp.concatenate(tails, axis=1).astype(bf16)
    out_ref[:, GATE_AT:DOWN_AT] = gate_ref[:, :MAIN]
    out_ref[:, DOWN_AT : DOWN_AT + MAIN] = down_ref[:, :MAIN]
    tails = [down_ref[:, MAIN:].astype(f32), jnp.zeros((out_ref.shape[0], rest), f32)]
    out_ref[:, DOWN_AT + MAIN :] = jnp.concatenate(tails, axis=1).astype(bf16)


def gated(inner, gate, taps):
    length = gate.shape[0]
    at = iota(gate.shape, 0)
    main = inner[:length]
    after_edge = inner[length : length + 1]
    before_edge = inner[length + 1 : length + 2]
    earlier = jnp.where(at == 0, before_edge, pltpu.roll(main, 1, 0))
    later = jnp.where(at == length - 1, after_edge, pltpu.roll(main, length - 1, 0))
    conv = taps[0:1] * earlier + taps[1:2] * main + taps[2:3] * later
    return jax.nn.gelu(conv) * gate


def feed_kernel(
    core_ref,
    tokens_ref,
    edges_ref,
    weight_ref,
    taps_ref,
    own_ref,
    other_ref,
    rows_ref,
    loaded_ref,
    hidden_ref,
    sems,
):
    length, width = tokens_ref.shape
    pairs, own, _ = own_ref.shape

    def keep(hidden, cols):
        for x in range(pairs):
            for c in range(2):
                slot = core_ref[0] if c == 0 else 1 - core_ref[0]
                at = pl.multiple_of(slot * (pairs * own) + x * own, own)
                row = (2 * x + c) * own
                hidden_ref[pl.ds(at, own), cols] = hidden[row : row + own].astype(bf16)

    step = width // FEED_STEPS
    copies = []
    for i in range(FEED_STEPS + 1):
        place = (pl.ds(i * step, step), pl.ds(0, DOWN_AT))
        if i == FEED_STEPS:
            place = (pl.ds(0, width), pl.ds(DOWN_AT, PACKED - DOWN_AT))
        copies.append(
            pltpu.make_async_copy(weight_ref.at[place], loaded_ref.at[place], sems.at[i])
        )
        copies[i].start()
    rows_ref[:length, :] = tokens_ref[...]
    rows_ref[length:, :] = edges_ref[...]
    inner, gate = None, None
    for i in range(FEED_STEPS - 1):
        copies[i].wait()
        rows = slice(i * step, (i + 1) * step)
        left = rows_ref[:, rows]
        first = dot(left, loaded_ref[rows, :GATE_AT])
        second = dot(left[:length], loaded_ref[rows, GATE_AT:DOWN_AT])
        inner = first if inner is None else inner + first
        gate = second if gate is None else gate + second
    copies[FEED_STEPS - 1].wait()
    rows = slice(width - step, width)
    left = rows_ref[:, rows]
    for at in range(0, GATE_AT, FEED_COLS):
        end = at + FEED_COLS
        stop = min(end, MAIN)
        up = inner[:, at:end] + dot(left, loaded_ref[rows, at:end])
        weight = loaded_ref[rows, GATE_AT + at : GATE_AT + stop]
        by = gate[:, at:stop] + dot(left[:length], weight)
        rounded = up.astype(bf16).astype(f32)
        keep(gated(rounded[:, : stop - at], by, taps_ref[:, at:stop]), slice(at, stop))
        if end > MAIN:
            by = pltpu.roll(up[:length, stop - at :], 64, 1)
            hidden = gated(rounded[:, stop - at :], by, taps_ref[:, MAIN:])
            hidden = jnp.where(iota(hidden.shape, 1) < HIDDEN - MAIN, hidden, 0.0)
            keep(hidden, slice(MAIN, None))
    copies[FEED_STEPS].wait()
    for at in range(0, width, 256):
        cols = slice(at, at + 256)
        part = dot(hidden_ref[...], loaded_ref[cols, DOWN_AT:], ((1,), (1,))).astype(bf16)
        own_ref[:, :, cols] = part[: length // 2].reshape(pairs, own, 256)
        other_ref[:, :, cols] = part[length // 2 :].reshape(pairs, own, 256)


def near(x):
    return pltpu.with_memory_space_constraint(x, pltpu.VMEM)


def whole_call(kernel, out_shape, in_specs, name):
    def call(*args):
        return pl.pallas_call(
            kernel,
            out_shape=out_shape,
            in_specs=in_specs,
            out_specs=jax.tree.map(lambda _: VMEM, out_shape),
            name=name,
        )(*args)

    return call


def shape_of(dims, dtype):
    return jax.ShapeDtypeStruct(dims, dtype)


def exchanged(pieces, axis):
    return lax.all_to_all(pieces, axis, split_axis=0, concat_axis=0, tiled=True)


def body(
    lookup_request_vectors,
    lookup_address_vectors,
    lookup_content_vectors,
    admission_preactivation,
    retention_preactivation,
    extra_decay_terms,
    per_slot_rescale_factor,
    mixer_exit_matrix,
    skip_path_activity,
    mlp_rescale_factor,
    filter_widening_matrix,
    multiplier_widening_matrix,
    neighbour_filter_coefficients,
    contracting_matrix,
):
    length = lookup_request_vectors.shape[0]
    width = mixer_exit_matrix.shape[1]
    members = lax.axis_size(TP)

    packed = whole_call(
        pack_kernel, shape_of((filter_widening_matrix.shape[0], PACKED), bf16), [VMEM] * 3, "pack"
    )(filter_widening_matrix, multiplier_widening_matrix, contracting_matrix.T)
    weights = lax.all_gather(packed, SP, axis=0, tiled=True)

    decay = jax.nn.log_sigmoid(retention_preactivation) + extra_decay_terms
    rate = admission_preactivation

    row, column = lax.axis_index("sp_0").reshape(1), "sp_1"
    pieces = pltpu.VMEM((8, 24, LANES), f32)
    summary = whole_call(summarize_kernel, pieces, [VMEM] * 4, "summarize")(
        lookup_address_vectors, lookup_content_vectors, rate, decay
    )
    along, inside = whole_call(
        along_kernel,
        (pltpu.VMEM((8, 16, LANES), f32), pltpu.VMEM((8, 24, LANES), f32)),
        [SMEM, VMEM],
        "along",
    )(row, near(exchanged(summary, column)))
    across = whole_call(across_kernel, pieces, [SMEM, VMEM, VMEM], "across")(
        row, near(exchanged(along, "sp_0")), near(inside)
    )
    partial_out = whole_call(
        mix_kernel, pltpu.VMEM((length, width), bf16), [VMEM] * 8, "mix"
    )(
        near(exchanged(across, column)),
        lookup_request_vectors,
        lookup_address_vectors,
        lookup_content_vectors,
        rate,
        decay,
        per_slot_rescale_factor.reshape(1, LANES),
        mixer_exit_matrix,
    )
    own = length // members
    pieces = near(exchanged(partial_out.reshape(members, own, width), TP))
    middle, normed = whole_call(
        norm_kernel,
        (shape_of((own, width), bf16), pltpu.VMEM((members, own, width), bf16)),
        [VMEM] * 3,
        "norm",
    )(pieces, skip_path_activity, mlp_rescale_factor.reshape(1, width))
    tokens = exchanged(normed, TP).reshape(length, width)

    peers = lax.axis_size(SP)
    up = [(i, i + 1) for i in range(peers - 1)]
    down = [(j, i) for i, j in up]
    earlier = lax.ppermute(tokens[length - 1 :], SP, up)
    later = lax.ppermute(tokens[:1], SP, down)
    edges = jnp.concatenate([later, earlier, jnp.zeros((14, width), bf16)], axis=0)

    halves = pltpu.VMEM((members // 2, own, width), bf16)
    own_half, other_half = pl.pallas_call(
        feed_kernel,
        out_shape=(halves, halves),
        in_specs=[SMEM, VMEM, VMEM, ANY, VMEM],
        out_specs=(VMEM, VMEM),
        scratch_shapes=[
            pltpu.VMEM((length + 16, width), bf16),
            pltpu.VMEM((width, PACKED), bf16),
            pltpu.VMEM((length, 768), bf16),
            pltpu.SemaphoreType.DMA((FEED_STEPS + 1,)),
        ],
        name="feed",
    )(
        lax.axis_index("core").reshape(1),
        near(tokens),
        near(edges),
        pltpu.with_memory_space_constraint(weights, pltpu.HBM),
        jnp.pad(neighbour_filter_coefficients, ((0, 0), (0, 768 - HIDDEN))),
    )
    from_partner = lax.ppermute(other_half, "core", [(0, 1), (1, 0)])
    pair = (own_half.astype(f32) + from_partner.astype(f32)).astype(bf16)
    pieces = exchanged(pair, "x").astype(f32)
    total = middle.astype(f32)
    for j in range(pieces.shape[0]):
        total = total + pieces[j]
    return total.astype(bf16)


def solution(mesh):
    split = Mesh(mesh.devices.reshape(8, 8, 4, 2), SP_TP)
    placed = (
        P(SP, TP),
        P(SP, TP),
        P(SP, TP),
        P(None, TP, SP),
        P(None, TP, SP),
        P(None, TP, SP),
        P(TP),
        P(TP, None),
        P(SP_TP, None),
        P(),
        P(SP, TP),
        P(SP, TP),
        P(None, TP),
        P(TP, SP),
    )
    return jax.shard_map(
        body, mesh=split, in_specs=placed, out_specs=P(SP_TP, None), check_vma=False
    )
```

```python
import jax
import jax.numpy as jnp
from jax import lax
from jax.experimental import pallas as pl
from jax.experimental.pallas import tpu as pltpu
from jax.sharding import Mesh
from jax.sharding import PartitionSpec as P

HEAD_DIM = 64
SP = ("sp_0", "sp_1")
TP = ("x", "core")
SP_TP = SP + TP
EPS = 1e-06
FAR_BELOW = -1e30
LANES = 128
HIDDEN = 704
MAIN = 640
GATE_AT = MAIN + 128
DOWN_AT = GATE_AT + MAIN
PACKED = DOWN_AT + 768
FEED_STEPS = 2
FEED_COLS = 256
ANY = pl.BlockSpec(memory_space=pl.ANY)
f32 = jnp.float32
bf16 = jnp.bfloat16
VMEM = pl.BlockSpec(memory_space=pltpu.VMEM)
SMEM = pl.BlockSpec(memory_space=pltpu.SMEM)


def three_parts(x):
    hi = x.astype(bf16)
    rest = x - hi.astype(f32)
    mid = rest.astype(bf16)
    low = (rest - mid.astype(f32)).astype(bf16)
    return hi, mid, low


def dot(a, b, dims=((1,), (0,))):
    return lax.dot_general(a, b, (dims, ((), ())), preferred_element_type=f32)


def dot_parts(parts, b, dims=((1,), (0,))):
    total = dot(parts[0], b, dims)
    for part in parts[1:]:
        total = total + dot(part, b, dims)
    return total


def iota(shape, dim):
    return lax.broadcasted_iota(jnp.int32, shape, dim)


def gate_rows(ref):
    place = iota((8, ref.shape[2]), 0)
    out = jnp.zeros((8, ref.shape[2]), f32)
    for d in range(2):
        for h in range(2):
            out = jnp.where(place == 2 * d + h, ref[d, h : h + 1, :], out)
    return out


def by_head(first, second, shape):
    return jnp.where(iota(shape, len(shape) - 1) < HEAD_DIM, first, second)


def packed_rows(rows, count):
    place = iota((count, LANES), 0)
    out = jnp.zeros((count, LANES), f32)
    for k, row in enumerate(rows):
        out = jnp.where(place == k, row, out)
    return out


def nothing(rows):
    line = jnp.zeros((1, LANES), f32)
    return line, jnp.zeros((rows, LANES), f32), line, jnp.full((1, LANES), FAR_BELOW, f32)


def combined(earlier, later):
    total_a, memory_a, normal_a, top_a = earlier
    total_b, memory_b, normal_b, top_b = later
    lifted = total_b + top_a
    top = jnp.maximum(lifted, top_b)
    weight_a, weight_b = jnp.exp(lifted - top), jnp.exp(top_b - top)
    memory = weight_a * memory_a + weight_b * memory_b
    return total_a + total_b, memory, weight_a * normal_a + weight_b * normal_b, top


def in_order(d, peers):
    return range(peers) if d == 0 else reversed(range(peers))


def summarize_kernel(key_ref, value_ref, rate_ref, decay_ref, out_ref):
    length = key_ref.shape[0]
    rate = gate_rows(rate_ref)
    decay = gate_rows(decay_ref)
    upper = (iota((length, length), 0) <= iota((length, length), 1)).astype(bf16)
    cumul = dot_parts(three_parts(decay), upper)
    total = cumul[:, length - 1 : length]
    is_forward = iota((8, length), 0) < 2
    weight = jnp.where(is_forward, total - cumul, cumul - decay) + rate
    top = jnp.max(weight, axis=1, keepdims=True)
    fresh = jnp.exp(weight - top)
    key_t = key_ref[...].astype(f32).T * HEAD_DIM ** (-0.5)
    value = value_ref[...]
    normal_all = dot_parts(three_parts(fresh), key_ref[...]) * HEAD_DIM ** (-0.5)
    memories, normals, totals, tops = [], [], [], []
    for d in range(2):
        a, b = 2 * d, 2 * d + 1
        spread = jnp.concatenate(
            [
                jnp.broadcast_to(fresh[a : a + 1], (HEAD_DIM, length)),
                jnp.broadcast_to(fresh[b : b + 1], (HEAD_DIM, length)),
            ],
            axis=0,
        )
        both = dot_parts(three_parts(key_t * spread), value)
        memories.append(by_head(both[:HEAD_DIM], both[HEAD_DIM:], (HEAD_DIM, LANES)))
        row = (1, LANES)
        normals.append(by_head(normal_all[a : a + 1], normal_all[b : b + 1], row))
        totals.append(by_head(total[a : a + 1], total[b : b + 1], row))
        tops.append(by_head(top[a : a + 1], top[b : b + 1], row))
    tail = packed_rows([*normals, *totals, *tops], 8)
    for j in range(out_ref.shape[0]):
        part = [memory[8 * j : 8 * (j + 1)] for memory in memories]
        out_ref[j, :16, :] = jnp.concatenate(part, axis=0)
        out_ref[j, 16:, :] = tail


def along_kernel(here_ref, pieces_ref, out_ref, inside_ref):
    peers = pieces_ref.shape[0]
    tails = [pieces_ref[j, 16:, :] for j in range(peers)]
    memories = [pieces_ref[j, :16, :] for j in range(peers)]
    reaching = []
    wholes = []
    for d in range(2):
        state = nothing(8)
        reached = {}
        for j in in_order(d, peers):
            reached[j] = state
            normal, total, top = (tails[j][d + k : d + k + 1] for k in (0, 2, 4))
            state = combined(state, (total, memories[j][8 * d : 8 * (d + 1)], normal, top))
        reaching.append(reached)
        total, memory, normal, top = state
        rows = packed_rows([normal, total, top], 8)
        wholes.append(jnp.concatenate([memory, rows], axis=0))
    for j in range(peers):
        lines = []
        for d in range(2):
            total, memory, normal, top = reaching[d][j]
            inside_ref[j, 8 * d : 8 * (d + 1), :] = memory
            lines += [total, normal, top]
        inside_ref[j, 16:, :] = packed_rows(lines, 8)
    for j in range(out_ref.shape[0]):
        out_ref[j] = jnp.where(j > here_ref[0], wholes[0], wholes[1])


def across_kernel(here_ref, pieces_ref, inside_ref, out_ref):
    peers = pieces_ref.shape[0]
    here = here_ref[0]
    far = []
    for d in range(2):
        state = nothing(8)
        for j in in_order(d, peers):
            piece = pieces_ref[j]
            later = (piece[9:10], piece[:8], piece[8:9], piece[10:11])
            on = j < here if d == 0 else j > here
            state = [jnp.where(on, x, y) for x, y in zip(combined(state, later), state)]
        far.append(state)
    for j in range(out_ref.shape[0]):
        memories, normals, tops = [], [], []
        lines = inside_ref[j, 16:, :]
        for d in range(2):
            total, normal, top = (lines[3 * d + k : 3 * d + k + 1] for k in range(3))
            near_state = (total, inside_ref[j, 8 * d : 8 * (d + 1), :], normal, top)
            _, memory, normal, top = combined(far[d], near_state)
            memories.append(memory)
            normals.append(normal)
            tops.append(top)
        out_ref[j, :16, :] = jnp.concatenate(memories, axis=0)
        out_ref[j, 16:, :] = packed_rows(normals + tops, 8)


def head_sums(x, shape):
    first = iota(shape, 1) < HEAD_DIM
    a = jnp.sum(jnp.where(first, x, 0.0), axis=1, keepdims=True)
    b = jnp.sum(jnp.where(first, 0.0, x), axis=1, keepdims=True)
    return a, b


def mix_kernel(
    pieces_ref,
    query_ref,
    key_ref,
    value_ref,
    rate_ref,
    decay_ref,
    gain_ref,
    exit_ref,
    out_ref,
):
    peers = pieces_ref.shape[0]
    tail = pieces_ref[0, 16:, :]
    length = query_ref.shape[0]
    wide = (length, LANES)
    query = query_ref[...]
    value = value_ref[...]
    query32 = query.astype(f32)
    rate = gate_rows(rate_ref)
    parts = three_parts(gate_rows(decay_ref))
    square = (length, length)
    row_at, lane_at = iota(square, 0), iota(square, 1)
    lane_head = iota((length, LANES), 1) // HEAD_DIM
    scores = []
    for h in range(2):
        own = jnp.where(lane_head == h, query32, 0.0).astype(bf16)
        scores.append(dot(own, key_ref[...], ((1,), (1,))) * HEAD_DIM ** (-0.5))
    summed = jnp.zeros(wide, f32)
    for d in range(2):
        memory = jnp.concatenate(
            [pieces_ref[j, 8 * d : 8 * (d + 1), :] for j in range(peers)], axis=0
        )
        normal, top_in = tail[d : d + 1], tail[2 + d : 3 + d]

        seen = row_at >= lane_at if d == 0 else row_at <= lane_at
        seen_t = (row_at <= lane_at if d == 0 else row_at >= lane_at).astype(bf16)
        cumul_rows = dot_parts(parts, seen_t)
        cumul_cols = dot_parts([seen.astype(bf16)], parts[0], ((1,), (1,)))
        for part in parts[1:]:
            cumul_cols = cumul_cols + dot(seen.astype(bf16), part, ((1,), (1,)))

        first = iota((HEAD_DIM, LANES), 1) < HEAD_DIM
        block = jnp.concatenate(
            [jnp.where(first, memory, 0.0), jnp.where(first, 0.0, memory)], axis=0
        )
        carried_out = sum(dot(query, part) for part in three_parts(block))
        carried_den = head_sums(query32 * normal, wide)

        numer, denom, carry = [], [], []
        for h in range(2):
            r = 2 * d + h
            at_query = cumul_cols[:, r : r + 1]
            spread = at_query + (rate[r : r + 1] - cumul_rows[r : r + 1])
            spread = jnp.where(seen, spread, -jnp.inf)
            carried = at_query + top_in[:, HEAD_DIM * h : HEAD_DIM * h + 1]
            row_top = jnp.maximum(carried, jnp.max(spread, axis=1, keepdims=True))
            weighted = scores[h] * jnp.exp(spread - row_top)
            carry_weight = jnp.exp(carried - row_top)
            numer.append(dot_parts(three_parts(weighted), value))
            total = jnp.sum(weighted, axis=1, keepdims=True) + carry_weight * carried_den[h]
            denom.append(jnp.maximum(jnp.abs(total), jnp.exp(-row_top)))
            carry.append(carry_weight)
        top_part = by_head(numer[0], numer[1], wide)
        top_part = top_part + by_head(carry[0], carry[1], wide) * carried_out
        summed = summed + top_part / by_head(denom[0], denom[1], wide)
    squares = head_sums(summed * summed, wide)
    mean = by_head(squares[0], squares[1], wide) * (1.0 / HEAD_DIM)
    mixed = (summed * lax.rsqrt(mean + EPS) * gain_ref[...]).astype(bf16)
    out_ref[...] = dot(mixed, exit_ref[...]).astype(bf16)


def norm_kernel(pieces_ref, skip_ref, gain_ref, middle_ref, normed_ref):
    total = skip_ref[...].astype(f32)
    projected = pieces_ref[0].astype(f32)
    for j in range(1, pieces_ref.shape[0]):
        projected = projected + pieces_ref[j].astype(f32)
    middle = (total + projected).astype(bf16)
    middle_ref[...] = middle
    wide = middle.astype(f32)
    mean = jnp.mean(wide * wide, axis=1, keepdims=True)
    normed = (wide * lax.rsqrt(mean + EPS) * gain_ref[...]).astype(bf16)
    for copy in range(normed_ref.shape[0]):
        normed_ref[copy] = normed


def pack_kernel(up_ref, gate_ref, down_ref, out_ref):
    rest = HIDDEN - MAIN
    out_ref[:, :MAIN] = up_ref[:, :MAIN]
    tails = [up_ref[:, MAIN:].astype(f32), gate_ref[:, MAIN:].astype(f32)]
    out_ref[:, MAIN:GATE_AT] = jnp.concatenate(tails, axis=1).astype(bf16)
    out_ref[:, GATE_AT:DOWN_AT] = gate_ref[:, :MAIN]
    out_ref[:, DOWN_AT : DOWN_AT + MAIN] = down_ref[:, :MAIN]
    tails = [down_ref[:, MAIN:].astype(f32), jnp.zeros((out_ref.shape[0], rest), f32)]
    out_ref[:, DOWN_AT + MAIN :] = jnp.concatenate(tails, axis=1).astype(bf16)


def gated(inner, gate, taps):
    length = gate.shape[0]
    at = iota(gate.shape, 0)
    main = inner[:length]
    after_edge = inner[length : length + 1]
    before_edge = inner[length + 1 : length + 2]
    earlier = jnp.where(at == 0, before_edge, pltpu.roll(main, 1, 0))
    later = jnp.where(at == length - 1, after_edge, pltpu.roll(main, length - 1, 0))
    conv = taps[0:1] * earlier + taps[1:2] * main + taps[2:3] * later
    return jax.nn.gelu(conv) * gate


def feed_kernel(
    core_ref,
    tokens_ref,
    edges_ref,
    weight_ref,
    taps_ref,
    other_ref,
    hidden_ref,
    down_ref,
    rows_ref,
    loaded_ref,
    sems,
):
    length, width = tokens_ref.shape
    pairs, own, _ = other_ref.shape

    def keep(hidden, cols):
        for x in range(pairs):
            for c in range(2):
                slot = core_ref[0] if c == 0 else 1 - core_ref[0]
                at = pl.multiple_of(slot * (pairs * own) + x * own, own)
                row = (2 * x + c) * own
                hidden_ref[pl.ds(at, own), cols] = hidden[row : row + own].astype(bf16)

    step = width // FEED_STEPS
    copies = []
    for i in range(FEED_STEPS + 1):
        place, target = (pl.ds(i * step, step), pl.ds(0, DOWN_AT)), loaded_ref
        if i == FEED_STEPS:
            place, target = (pl.ds(0, width), pl.ds(DOWN_AT, PACKED - DOWN_AT)), down_ref
        target = target if i == FEED_STEPS else target.at[place]
        copies.append(pltpu.make_async_copy(weight_ref.at[place], target, sems.at[i]))
        copies[i].start()
    rows_ref[:length, :] = tokens_ref[...]
    rows_ref[length:, :] = edges_ref[...]
    inner, gate = None, None
    for i in range(FEED_STEPS - 1):
        copies[i].wait()
        rows = slice(i * step, (i + 1) * step)
        left = rows_ref[:, rows]
        first = dot(left, loaded_ref[rows, :GATE_AT])
        second = dot(left[:length], loaded_ref[rows, GATE_AT:DOWN_AT])
        inner = first if inner is None else inner + first
        gate = second if gate is None else gate + second
    copies[FEED_STEPS - 1].wait()
    rows = slice(width - step, width)
    left = rows_ref[:, rows]
    for at in range(0, GATE_AT, FEED_COLS):
        end = at + FEED_COLS
        stop = min(end, MAIN)
        up = inner[:, at:end] + dot(left, loaded_ref[rows, at:end])
        weight = loaded_ref[rows, GATE_AT + at : GATE_AT + stop]
        by = gate[:, at:stop] + dot(left[:length], weight)
        rounded = up.astype(bf16).astype(f32)
        keep(gated(rounded[:, : stop - at], by, taps_ref[:, at:stop]), slice(at, stop))
        if end > MAIN:
            by = pltpu.roll(up[:length, stop - at :], 64, 1)
            hidden = gated(rounded[:, stop - at :], by, taps_ref[:, MAIN:])
            hidden = jnp.where(iota(hidden.shape, 1) < HIDDEN - MAIN, hidden, 0.0)
            keep(hidden, slice(MAIN, None))
    copies[FEED_STEPS].wait()
    lowered(other_ref, hidden_ref[length // 2 :, :], down_ref)


def lowered(out_ref, hidden, down_ref):
    for at in range(0, down_ref.shape[0], 256):
        cols = slice(at, at + 256)
        part = dot(hidden, down_ref[cols, :], ((1,), (1,))).astype(bf16)
        out_ref[:, :, cols] = part.reshape(out_ref.shape[0], out_ref.shape[1], 256)


def own_kernel(hidden_ref, down_ref, out_ref):
    lowered(out_ref, hidden_ref[: hidden_ref.shape[0] // 2, :], down_ref)


def near(x):
    return pltpu.with_memory_space_constraint(x, pltpu.VMEM)


def whole_call(kernel, out_shape, in_specs, name):
    def call(*args):
        return pl.pallas_call(
            kernel,
            out_shape=out_shape,
            in_specs=in_specs,
            out_specs=jax.tree.map(lambda _: VMEM, out_shape),
            name=name,
        )(*args)

    return call


def shape_of(dims, dtype):
    return jax.ShapeDtypeStruct(dims, dtype)


def exchanged(pieces, axis):
    return lax.all_to_all(pieces, axis, split_axis=0, concat_axis=0, tiled=True)


def body(
    lookup_request_vectors,
    lookup_address_vectors,
    lookup_content_vectors,
    admission_preactivation,
    retention_preactivation,
    extra_decay_terms,
    per_slot_rescale_factor,
    mixer_exit_matrix,
    skip_path_activity,
    mlp_rescale_factor,
    filter_widening_matrix,
    multiplier_widening_matrix,
    neighbour_filter_coefficients,
    contracting_matrix,
):
    length = lookup_request_vectors.shape[0]
    width = mixer_exit_matrix.shape[1]
    members = lax.axis_size(TP)

    packed = whole_call(
        pack_kernel, shape_of((filter_widening_matrix.shape[0], PACKED), bf16), [VMEM] * 3, "pack"
    )(filter_widening_matrix, multiplier_widening_matrix, contracting_matrix.T)
    weights = lax.all_gather(packed, SP, axis=0, tiled=True)

    decay = jax.nn.log_sigmoid(retention_preactivation) + extra_decay_terms
    rate = admission_preactivation

    row, column = lax.axis_index("sp_0").reshape(1), "sp_1"
    pieces = pltpu.VMEM((8, 24, LANES), f32)
    summary = whole_call(summarize_kernel, pieces, [VMEM] * 4, "summarize")(
        lookup_address_vectors, lookup_content_vectors, rate, decay
    )
    along, inside = whole_call(
        along_kernel,
        (pltpu.VMEM((8, 16, LANES), f32), pltpu.VMEM((8, 24, LANES), f32)),
        [SMEM, VMEM],
        "along",
    )(row, near(exchanged(summary, column)))
    across = whole_call(across_kernel, pieces, [SMEM, VMEM, VMEM], "across")(
        row, near(exchanged(along, "sp_0")), near(inside)
    )
    partial_out = whole_call(
        mix_kernel, pltpu.VMEM((length, width), bf16), [VMEM] * 8, "mix"
    )(
        near(exchanged(across, column)),
        lookup_request_vectors,
        lookup_address_vectors,
        lookup_content_vectors,
        rate,
        decay,
        per_slot_rescale_factor.reshape(1, LANES),
        mixer_exit_matrix,
    )
    own = length // members
    pieces = near(exchanged(partial_out.reshape(members, own, width), TP))
    middle, normed = whole_call(
        norm_kernel,
        (shape_of((own, width), bf16), pltpu.VMEM((members, own, width), bf16)),
        [VMEM] * 3,
        "norm",
    )(pieces, skip_path_activity, mlp_rescale_factor.reshape(1, width))
    tokens = exchanged(normed, TP).reshape(length, width)

    peers = lax.axis_size(SP)
    up = [(i, i + 1) for i in range(peers - 1)]
    down = [(j, i) for i, j in up]
    earlier = lax.ppermute(tokens[length - 1 :], SP, up)
    later = lax.ppermute(tokens[:1], SP, down)
    edges = jnp.concatenate([later, earlier, jnp.zeros((14, width), bf16)], axis=0)

    halves = pltpu.VMEM((members // 2, own, width), bf16)
    other_half, hidden, down_part = pl.pallas_call(
        feed_kernel,
        out_shape=(
            halves,
            pltpu.VMEM((length, 768), bf16),
            pltpu.VMEM((width, PACKED - DOWN_AT), bf16),
        ),
        in_specs=[SMEM, VMEM, VMEM, ANY, VMEM],
        out_specs=(VMEM, VMEM, VMEM),
        scratch_shapes=[
            pltpu.VMEM((length + 16, width), bf16),
            pltpu.VMEM((width, DOWN_AT), bf16),
            pltpu.SemaphoreType.DMA((FEED_STEPS + 1,)),
        ],
        compiler_params=pltpu.CompilerParams(vmem_limit_bytes=40 * 2**20),
        name="feed",
    )(
        lax.axis_index("core").reshape(1),
        near(tokens),
        near(edges),
        pltpu.with_memory_space_constraint(weights, pltpu.HBM),
        jnp.pad(neighbour_filter_coefficients, ((0, 0), (0, 768 - HIDDEN))),
    )
    from_partner = lax.ppermute(other_half, "core", [(0, 1), (1, 0)])
    own_half = pl.pallas_call(
        own_kernel,
        out_shape=halves,
        in_specs=[VMEM] * 2,
        out_specs=VMEM,
        compiler_params=pltpu.CompilerParams(vmem_limit_bytes=40 * 2**20),
        name="own",
    )(near(hidden), near(down_part))
    pair = (own_half.astype(f32) + from_partner.astype(f32)).astype(bf16)
    pieces = exchanged(pair, "x").astype(f32)
    total = middle.astype(f32)
    for j in range(pieces.shape[0]):
        total = total + pieces[j]
    return total.astype(bf16)


def solution(mesh):
    split = Mesh(mesh.devices.reshape(8, 8, 4, 2), SP_TP)
    placed = (
        P(SP, TP),
        P(SP, TP),
        P(SP, TP),
        P(None, TP, SP),
        P(None, TP, SP),
        P(None, TP, SP),
        P(TP),
        P(TP, None),
        P(SP_TP, None),
        P(),
        P(SP, TP),
        P(SP, TP),
        P(None, TP),
        P(TP, SP),
    )
    return jax.shard_map(
        body, mesh=split, in_specs=placed, out_specs=P(SP_TP, None), check_vma=False
    )
```

```python
import jax
import jax.numpy as jnp
from jax import lax
from jax.experimental import pallas as pl
from jax.experimental.pallas import tpu as pltpu
from jax.sharding import Mesh
from jax.sharding import PartitionSpec as P

HEAD_DIM = 64
SP = ("sp_0", "sp_1")
TP = ("x", "core")
SP_TP = SP + TP
EPS = 1e-06
FAR_BELOW = -1e30
LANES = 128
HIDDEN = 704
MAIN = 640
GATE_AT = MAIN + 128
DOWN_AT = GATE_AT + MAIN
PACKED = DOWN_AT + 768
FEED_STEPS = 2
FEED_COLS = 256
ANY = pl.BlockSpec(memory_space=pl.ANY)
f32 = jnp.float32
bf16 = jnp.bfloat16
VMEM = pl.BlockSpec(memory_space=pltpu.VMEM)
SMEM = pl.BlockSpec(memory_space=pltpu.SMEM)


def three_parts(x):
    hi = x.astype(bf16)
    rest = x - hi.astype(f32)
    mid = rest.astype(bf16)
    low = (rest - mid.astype(f32)).astype(bf16)
    return hi, mid, low


def dot(a, b, dims=((1,), (0,))):
    return lax.dot_general(a, b, (dims, ((), ())), preferred_element_type=f32)


def dot_parts(parts, b, dims=((1,), (0,))):
    total = dot(parts[0], b, dims)
    for part in parts[1:]:
        total = total + dot(part, b, dims)
    return total


def iota(shape, dim):
    return lax.broadcasted_iota(jnp.int32, shape, dim)


def gate_rows(ref):
    place = iota((8, ref.shape[2]), 0)
    out = jnp.zeros((8, ref.shape[2]), f32)
    for d in range(2):
        for h in range(2):
            out = jnp.where(place == 2 * d + h, ref[d, h : h + 1, :], out)
    return out


def by_head(first, second, shape):
    return jnp.where(iota(shape, len(shape) - 1) < HEAD_DIM, first, second)


def packed_rows(rows, count):
    place = iota((count, LANES), 0)
    out = jnp.zeros((count, LANES), f32)
    for k, row in enumerate(rows):
        out = jnp.where(place == k, row, out)
    return out


def nothing(rows):
    line = jnp.zeros((1, LANES), f32)
    return line, jnp.zeros((rows, LANES), f32), line, jnp.full((1, LANES), FAR_BELOW, f32)


def combined(earlier, later):
    total_a, memory_a, normal_a, top_a = earlier
    total_b, memory_b, normal_b, top_b = later
    lifted = total_b + top_a
    top = jnp.maximum(lifted, top_b)
    weight_a, weight_b = jnp.exp(lifted - top), jnp.exp(top_b - top)
    memory = weight_a * memory_a + weight_b * memory_b
    return total_a + total_b, memory, weight_a * normal_a + weight_b * normal_b, top


def in_order(d, peers):
    return range(peers) if d == 0 else reversed(range(peers))


def summarize_kernel(key_ref, value_ref, rate_ref, decay_ref, out_ref):
    length = key_ref.shape[0]
    rate = gate_rows(rate_ref)
    decay = gate_rows(decay_ref)
    upper = (iota((length, length), 0) <= iota((length, length), 1)).astype(bf16)
    cumul = dot_parts(three_parts(decay), upper)
    total = cumul[:, length - 1 : length]
    is_forward = iota((8, length), 0) < 2
    weight = jnp.where(is_forward, total - cumul, cumul - decay) + rate
    top = jnp.max(weight, axis=1, keepdims=True)
    fresh = jnp.exp(weight - top)
    key_t = key_ref[...].astype(f32).T * HEAD_DIM ** (-0.5)
    value = value_ref[...]
    normal_all = dot_parts(three_parts(fresh), key_ref[...]) * HEAD_DIM ** (-0.5)
    memories, normals, totals, tops = [], [], [], []
    for d in range(2):
        a, b = 2 * d, 2 * d + 1
        spread = jnp.concatenate(
            [
                jnp.broadcast_to(fresh[a : a + 1], (HEAD_DIM, length)),
                jnp.broadcast_to(fresh[b : b + 1], (HEAD_DIM, length)),
            ],
            axis=0,
        )
        both = dot_parts(three_parts(key_t * spread), value)
        memories.append(by_head(both[:HEAD_DIM], both[HEAD_DIM:], (HEAD_DIM, LANES)))
        row = (1, LANES)
        normals.append(by_head(normal_all[a : a + 1], normal_all[b : b + 1], row))
        totals.append(by_head(total[a : a + 1], total[b : b + 1], row))
        tops.append(by_head(top[a : a + 1], top[b : b + 1], row))
    tail = packed_rows([*normals, *totals, *tops], 8)
    for j in range(out_ref.shape[0]):
        part = [memory[8 * j : 8 * (j + 1)] for memory in memories]
        out_ref[j, :16, :] = jnp.concatenate(part, axis=0)
        out_ref[j, 16:, :] = tail


def along_kernel(here_ref, pieces_ref, out_ref, inside_ref):
    peers = pieces_ref.shape[0]
    tails = [pieces_ref[j, 16:, :] for j in range(peers)]
    memories = [pieces_ref[j, :16, :] for j in range(peers)]
    reaching = []
    wholes = []
    for d in range(2):
        state = nothing(8)
        reached = {}
        for j in in_order(d, peers):
            reached[j] = state
            normal, total, top = (tails[j][d + k : d + k + 1] for k in (0, 2, 4))
            state = combined(state, (total, memories[j][8 * d : 8 * (d + 1)], normal, top))
        reaching.append(reached)
        total, memory, normal, top = state
        rows = packed_rows([normal, total, top], 8)
        wholes.append(jnp.concatenate([memory, rows], axis=0))
    for j in range(peers):
        lines = []
        for d in range(2):
            total, memory, normal, top = reaching[d][j]
            inside_ref[j, 8 * d : 8 * (d + 1), :] = memory
            lines += [total, normal, top]
        inside_ref[j, 16:, :] = packed_rows(lines, 8)
    for j in range(out_ref.shape[0]):
        out_ref[j] = jnp.where(j > here_ref[0], wholes[0], wholes[1])


def across_kernel(here_ref, pieces_ref, inside_ref, out_ref):
    peers = pieces_ref.shape[0]
    here = here_ref[0]
    far = []
    for d in range(2):
        state = nothing(8)
        for j in in_order(d, peers):
            piece = pieces_ref[j]
            later = (piece[9:10], piece[:8], piece[8:9], piece[10:11])
            on = j < here if d == 0 else j > here
            state = [jnp.where(on, x, y) for x, y in zip(combined(state, later), state)]
        far.append(state)
    for j in range(out_ref.shape[0]):
        memories, normals, tops = [], [], []
        lines = inside_ref[j, 16:, :]
        for d in range(2):
            total, normal, top = (lines[3 * d + k : 3 * d + k + 1] for k in range(3))
            near_state = (total, inside_ref[j, 8 * d : 8 * (d + 1), :], normal, top)
            _, memory, normal, top = combined(far[d], near_state)
            memories.append(memory)
            normals.append(normal)
            tops.append(top)
        out_ref[j, :16, :] = jnp.concatenate(memories, axis=0)
        out_ref[j, 16:, :] = packed_rows(normals + tops, 8)


def head_sums(x, shape):
    first = iota(shape, 1) < HEAD_DIM
    a = jnp.sum(jnp.where(first, x, 0.0), axis=1, keepdims=True)
    b = jnp.sum(jnp.where(first, 0.0, x), axis=1, keepdims=True)
    return a, b


def mix_kernel(
    pieces_ref,
    query_ref,
    key_ref,
    value_ref,
    rate_ref,
    decay_ref,
    gain_ref,
    exit_ref,
    out_ref,
):
    peers = pieces_ref.shape[0]
    tail = pieces_ref[0, 16:, :]
    length = query_ref.shape[0]
    wide = (length, LANES)
    query = query_ref[...]
    value = value_ref[...]
    query32 = query.astype(f32)
    rate = gate_rows(rate_ref)
    parts = three_parts(gate_rows(decay_ref))
    square = (length, length)
    row_at, lane_at = iota(square, 0), iota(square, 1)
    lane_head = iota((length, LANES), 1) // HEAD_DIM
    scores = []
    for h in range(2):
        own = jnp.where(lane_head == h, query32, 0.0).astype(bf16)
        scores.append(dot(own, key_ref[...], ((1,), (1,))) * HEAD_DIM ** (-0.5))
    summed = jnp.zeros(wide, f32)
    for d in range(2):
        memory = jnp.concatenate(
            [pieces_ref[j, 8 * d : 8 * (d + 1), :] for j in range(peers)], axis=0
        )
        normal, top_in = tail[d : d + 1], tail[2 + d : 3 + d]

        seen = row_at >= lane_at if d == 0 else row_at <= lane_at
        seen_t = (row_at <= lane_at if d == 0 else row_at >= lane_at).astype(bf16)
        cumul_rows = dot_parts(parts, seen_t)
        cumul_cols = dot_parts([seen.astype(bf16)], parts[0], ((1,), (1,)))
        for part in parts[1:]:
            cumul_cols = cumul_cols + dot(seen.astype(bf16), part, ((1,), (1,)))

        first = iota((HEAD_DIM, LANES), 1) < HEAD_DIM
        block = jnp.concatenate(
            [jnp.where(first, memory, 0.0), jnp.where(first, 0.0, memory)], axis=0
        )
        carried_out = sum(dot(query, part) for part in three_parts(block))
        carried_den = head_sums(query32 * normal, wide)

        numer, denom, carry = [], [], []
        for h in range(2):
            r = 2 * d + h
            at_query = cumul_cols[:, r : r + 1]
            spread = at_query + (rate[r : r + 1] - cumul_rows[r : r + 1])
            spread = jnp.where(seen, spread, -jnp.inf)
            carried = at_query + top_in[:, HEAD_DIM * h : HEAD_DIM * h + 1]
            row_top = jnp.maximum(carried, jnp.max(spread, axis=1, keepdims=True))
            weighted = scores[h] * jnp.exp(spread - row_top)
            carry_weight = jnp.exp(carried - row_top)
            numer.append(dot_parts(three_parts(weighted), value))
            total = jnp.sum(weighted, axis=1, keepdims=True) + carry_weight * carried_den[h]
            denom.append(jnp.maximum(jnp.abs(total), jnp.exp(-row_top)))
            carry.append(carry_weight)
        top_part = by_head(numer[0], numer[1], wide)
        top_part = top_part + by_head(carry[0], carry[1], wide) * carried_out
        summed = summed + top_part / by_head(denom[0], denom[1], wide)
    squares = head_sums(summed * summed, wide)
    mean = by_head(squares[0], squares[1], wide) * (1.0 / HEAD_DIM)
    mixed = (summed * lax.rsqrt(mean + EPS) * gain_ref[...]).astype(bf16)
    out_ref[...] = dot(mixed, exit_ref[...]).astype(bf16)


def norm_kernel(pieces_ref, skip_ref, gain_ref, middle_ref, normed_ref):
    total = skip_ref[...].astype(f32)
    projected = pieces_ref[0].astype(f32)
    for j in range(1, pieces_ref.shape[0]):
        projected = projected + pieces_ref[j].astype(f32)
    middle = (total + projected).astype(bf16)
    middle_ref[...] = middle
    wide = middle.astype(f32)
    mean = jnp.mean(wide * wide, axis=1, keepdims=True)
    normed = (wide * lax.rsqrt(mean + EPS) * gain_ref[...]).astype(bf16)
    for copy in range(normed_ref.shape[0]):
        normed_ref[copy] = normed


def pack_kernel(up_ref, gate_ref, down_ref, out_ref):
    rest = HIDDEN - MAIN
    out_ref[:, :MAIN] = up_ref[:, :MAIN]
    tails = [up_ref[:, MAIN:].astype(f32), gate_ref[:, MAIN:].astype(f32)]
    out_ref[:, MAIN:GATE_AT] = jnp.concatenate(tails, axis=1).astype(bf16)
    out_ref[:, GATE_AT:DOWN_AT] = gate_ref[:, :MAIN]
    out_ref[:, DOWN_AT : DOWN_AT + MAIN] = down_ref[:, :MAIN]
    tails = [down_ref[:, MAIN:].astype(f32), jnp.zeros((out_ref.shape[0], rest), f32)]
    out_ref[:, DOWN_AT + MAIN :] = jnp.concatenate(tails, axis=1).astype(bf16)


def gated(inner, gate, taps):
    length = gate.shape[0]
    at = iota(gate.shape, 0)
    main = inner[:length]
    after_edge = inner[length : length + 1]
    before_edge = inner[length + 1 : length + 2]
    earlier = jnp.where(at == 0, before_edge, pltpu.roll(main, 1, 0))
    later = jnp.where(at == length - 1, after_edge, pltpu.roll(main, length - 1, 0))
    conv = taps[0:1] * earlier + taps[1:2] * main + taps[2:3] * later
    return jax.nn.gelu(conv) * gate


def feed_kernel(
    core_ref,
    tokens_ref,
    edges_ref,
    weight_ref,
    taps_ref,
    other_ref,
    hidden_ref,
    down_ref,
    rows_ref,
    loaded_ref,
    sems,
):
    length, width = tokens_ref.shape
    pairs, own, _ = other_ref.shape

    def keep(hidden, cols):
        for x in range(pairs):
            for c in range(2):
                slot = core_ref[0] if c == 0 else 1 - core_ref[0]
                at = pl.multiple_of(slot * (pairs * own) + x * own, own)
                row = (2 * x + c) * own
                hidden_ref[pl.ds(at, own), cols] = hidden[row : row + own].astype(bf16)

    step = width // FEED_STEPS
    copies = []
    for i in range(FEED_STEPS + 1):
        place, target = (pl.ds(i * step, step), pl.ds(0, DOWN_AT)), loaded_ref
        if i == FEED_STEPS:
            place, target = (pl.ds(0, width), pl.ds(DOWN_AT, PACKED - DOWN_AT)), down_ref
        target = target if i == FEED_STEPS else target.at[place]
        copies.append(pltpu.make_async_copy(weight_ref.at[place], target, sems.at[i]))
        copies[i].start()
    rows_ref[:length, :] = tokens_ref[...]
    rows_ref[length:, :] = edges_ref[...]
    inner, gate = None, None
    for i in range(FEED_STEPS - 1):
        copies[i].wait()
        rows = slice(i * step, (i + 1) * step)
        left = rows_ref[:, rows]
        first = dot(left, loaded_ref[rows, :GATE_AT])
        second = dot(left[:length], loaded_ref[rows, GATE_AT:DOWN_AT])
        inner = first if inner is None else inner + first
        gate = second if gate is None else gate + second
    copies[FEED_STEPS - 1].wait()
    rows = slice(width - step, width)
    left = rows_ref[:, rows]
    for at in range(0, GATE_AT, FEED_COLS):
        end = at + FEED_COLS
        stop = min(end, MAIN)
        up = inner[:, at:end] + dot(left, loaded_ref[rows, at:end])
        weight = loaded_ref[rows, GATE_AT + at : GATE_AT + stop]
        by = gate[:, at:stop] + dot(left[:length], weight)
        rounded = up.astype(bf16).astype(f32)
        keep(gated(rounded[:, : stop - at], by, taps_ref[:, at:stop]), slice(at, stop))
        if end > MAIN:
            by = pltpu.roll(up[:length, stop - at :], 64, 1)
            hidden = gated(rounded[:, stop - at :], by, taps_ref[:, MAIN:])
            hidden = jnp.where(iota(hidden.shape, 1) < HIDDEN - MAIN, hidden, 0.0)
            keep(hidden, slice(MAIN, None))
    copies[FEED_STEPS].wait()
    lowered(other_ref, hidden_ref[length // 2 :, :], down_ref)


def lowered(out_ref, hidden, down_ref):
    for at in range(0, down_ref.shape[0], 256):
        cols = slice(at, at + 256)
        part = dot(hidden, down_ref[cols, :], ((1,), (1,))).astype(bf16)
        out_ref[:, :, cols] = part.reshape(out_ref.shape[0], out_ref.shape[1], 256)


def own_kernel(hidden_ref, down_ref, out_ref):
    lowered(out_ref, hidden_ref[: hidden_ref.shape[0] // 2, :], down_ref)


def near(x):
    return pltpu.with_memory_space_constraint(x, pltpu.VMEM)


def whole_call(kernel, out_shape, in_specs, name):
    def call(*args):
        return pl.pallas_call(
            kernel,
            out_shape=out_shape,
            in_specs=in_specs,
            out_specs=jax.tree.map(lambda _: VMEM, out_shape),
            name=name,
        )(*args)

    return call


def shape_of(dims, dtype):
    return jax.ShapeDtypeStruct(dims, dtype)


def exchanged(pieces, axis):
    return lax.all_to_all(pieces, axis, split_axis=0, concat_axis=0, tiled=True)


def body(
    lookup_request_vectors,
    lookup_address_vectors,
    lookup_content_vectors,
    admission_preactivation,
    retention_preactivation,
    extra_decay_terms,
    per_slot_rescale_factor,
    mixer_exit_matrix,
    skip_path_activity,
    mlp_rescale_factor,
    filter_widening_matrix,
    multiplier_widening_matrix,
    neighbour_filter_coefficients,
    contracting_matrix,
):
    length = lookup_request_vectors.shape[0]
    width = mixer_exit_matrix.shape[1]
    members = lax.axis_size(TP)

    packed = whole_call(
        pack_kernel, shape_of((filter_widening_matrix.shape[0], PACKED), bf16), [VMEM] * 3, "pack"
    )(filter_widening_matrix, multiplier_widening_matrix, contracting_matrix.T)
    weights = lax.all_gather(packed, SP, axis=0, tiled=True)

    decay = jax.nn.log_sigmoid(retention_preactivation) + extra_decay_terms
    rate = admission_preactivation

    row, column = lax.axis_index("sp_0").reshape(1), "sp_1"
    pieces = pltpu.VMEM((8, 24, LANES), f32)
    summary = whole_call(summarize_kernel, pieces, [VMEM] * 4, "summarize")(
        lookup_address_vectors, lookup_content_vectors, rate, decay
    )
    along, inside = whole_call(
        along_kernel,
        (pltpu.VMEM((8, 16, LANES), f32), pltpu.VMEM((8, 24, LANES), f32)),
        [SMEM, VMEM],
        "along",
    )(row, near(exchanged(summary, column)))
    across = whole_call(across_kernel, pieces, [SMEM, VMEM, VMEM], "across")(
        row, near(exchanged(along, "sp_0")), near(inside)
    )
    partial_out = whole_call(
        mix_kernel, pltpu.VMEM((length, width), bf16), [VMEM] * 8, "mix"
    )(
        near(exchanged(across, column)),
        lookup_request_vectors,
        lookup_address_vectors,
        lookup_content_vectors,
        rate,
        decay,
        per_slot_rescale_factor.reshape(1, LANES),
        mixer_exit_matrix,
    )
    own = length // members
    pieces = near(exchanged(partial_out.reshape(members, own, width), TP))
    middle, normed = whole_call(
        norm_kernel,
        (shape_of((own, width), bf16), pltpu.VMEM((members, own, width), bf16)),
        [VMEM] * 3,
        "norm",
    )(pieces, skip_path_activity, mlp_rescale_factor.reshape(1, width))
    tokens = exchanged(normed, TP).reshape(length, width)

    peers = lax.axis_size(SP)
    up = [(i, i + 1) for i in range(peers - 1)]
    down = [(j, i) for i, j in up]
    earlier = lax.ppermute(tokens[length - 1 :], SP, up)
    later = lax.ppermute(tokens[:1], SP, down)
    edges = jnp.concatenate([later, earlier, jnp.zeros((14, width), bf16)], axis=0)

    halves = pltpu.VMEM((members // 2, own, width), bf16)
    other_half, hidden, down_part = pl.pallas_call(
        feed_kernel,
        out_shape=(
            halves,
            pltpu.VMEM((length, 768), bf16),
            pltpu.VMEM((width, PACKED - DOWN_AT), bf16),
        ),
        in_specs=[SMEM, VMEM, VMEM, ANY, VMEM],
        out_specs=(VMEM, VMEM, VMEM),
        scratch_shapes=[
            pltpu.VMEM((length + 16, width), bf16),
            pltpu.VMEM((width, DOWN_AT), bf16),
            pltpu.SemaphoreType.DMA((FEED_STEPS + 1,)),
        ],
        compiler_params=pltpu.CompilerParams(vmem_limit_bytes=40 * 2**20),
        name="feed",
    )(
        lax.axis_index("core").reshape(1),
        near(tokens),
        near(edges),
        pltpu.with_memory_space_constraint(weights, pltpu.HBM),
        jnp.pad(neighbour_filter_coefficients, ((0, 0), (0, 768 - HIDDEN))),
    )
    from_partner = lax.ppermute(other_half, "core", [(0, 1), (1, 0)])
    own_half = pl.pallas_call(
        own_kernel,
        out_shape=halves,
        in_specs=[VMEM] * 2,
        out_specs=VMEM,
        compiler_params=pltpu.CompilerParams(vmem_limit_bytes=40 * 2**20),
        name="own",
    )(near(hidden), near(down_part))
    pair = (own_half.astype(f32) + from_partner.astype(f32)).astype(bf16)
    pieces = exchanged(pair, "x")
    total = middle.astype(f32)
    for j in range(pieces.shape[0]):
        total = total + pieces[j].astype(f32)
    return total.astype(bf16)


def solution(mesh):
    split = Mesh(mesh.devices.reshape(8, 8, 4, 2), SP_TP)
    placed = (
        P(SP, TP),
        P(SP, TP),
        P(SP, TP),
        P(None, TP, SP),
        P(None, TP, SP),
        P(None, TP, SP),
        P(TP),
        P(TP, None),
        P(SP_TP, None),
        P(),
        P(SP, TP),
        P(SP, TP),
        P(None, TP),
        P(TP, SP),
    )
    return jax.shard_map(
        body, mesh=split, in_specs=placed, out_specs=P(SP_TP, None), check_vma=False
    )
```
